128 devices in a mesh: sp: 16 (over z, x), fs: 4 (over y), tp: 2 (over core).
Axes of the slice: x: 4, y: 4, z: 4, core: 2. Of those that a mesh axis runs over, the one named last changes fastest.
Arguments:
- inputs: bfloat16 [65536, 2048], P(('fs', 'sp'), 'tp'), parts along dimension 0, may hold values from -270 to 270
- mix_gain: float32 [2048], replicated, may hold values from 0.1 to 1.9
- w_query: bfloat16 [2048, 1024], P(None, 'tp'), may hold values from -0.125 to 0.125
- w_key: bfloat16 [2048, 256], P(None, 'tp'), may hold values from -0.125 to 0.125
- w_value: bfloat16 [2048, 256], P(None, 'tp'), may hold values from -0.125 to 0.125
- query_gain: float32 [64], replicated, may hold values from 0 to 14, as said below
- key_gain: float32 [64], replicated, may hold values from 0 to 14, as said below
- sink_logit: float32 [16], P('tp'), may hold values from 3 to 7
- w_inner: bfloat16 [2048, 1024], P(None, 'tp'), may hold values from -0.125 to 0.125
- w_bmat: bfloat16 [2048, 512], P(None, 'tp'), may hold values from -0.125 to 0.125
- w_cmat: bfloat16 [2048, 512], P(None, 'tp'), may hold values from -0.125 to 0.125
- w_gate: bfloat16 [2048, 1024], P(None, 'tp'), may hold values from -0.125 to 0.125
- w_step: bfloat16 [2048, 2, 16], P(None, None, 'tp'), may hold values from -0.125 to 0.125
- conv_inner: bfloat16 [5, 1024], P(None, 'tp'), may hold values from -2.5 to 2.5
- conv_bmat: bfloat16 [5, 512], P(None, 'tp'), may hold values from -2.5 to 2.5
- conv_cmat: bfloat16 [5, 512], P(None, 'tp'), may hold values from -2.5 to 2.5
- step_bias: float32 [2, 16], P(None, 'tp'), may hold values from -1 to 1
- decay_rate: float32 [2, 16], P(None, 'tp'), may hold values from 0 to 1, as said below
- decay_offset: float32 [16384, 2, 16], P('sp', None, 'tp'), may hold values from -3 to 0, as said below
- start_state: float32 [8, 16, 64, 128], P('fs', 'tp'), parts along dimension 0, may hold values from -192 to 192
- group_gain: float32 [1024], P('tp'), may hold values from 0.1 to 1.9
- w_out_attn: bfloat16 [1024, 2048], P('tp'), may hold values from -1.5 to 1.5
- w_out_state: bfloat16 [1024, 2048], P('tp'), may hold values from -0.1875 to 0.1875
Outputs:
- mixed: bfloat16 [65536, 2048], P(('fs', 'sp', 'tp')), parts along dimension 0
The draws below stay inside these ranges and needn't reach their ends.
There are 4 independent parts, one for each index of `fs`. The reference program is written for one: setup_inputs(seed, part) draws one part's arguments, and reference() takes and returns one part's arrays. A program takes and returns all parts, laid end to end along the dimension named above; an argument that names none is the same for every part. Nothing has to cross between parts.
Inputs may be any that keep to these rules, and one draw needn't show every extreme that they name: `query_gain`: positive. `key_gain`: positive. `decay_rate`: positive. `decay_offset`: never positive.
All inputs are finite; a program needn't handle non-finite values.
Results may differ from the reference program's by a relative error of at most 0.035.
Values may be sent and summed in bfloat16 or wider, within the bound.
No kernel may reach another device: no remote copies, remote signals or barrier semaphores. Data moves between devices by JAX's collectives and lax.ppermute only.
A program may use at most 128 MiB of HBM per device.

```python
import math
import jax
import jax.numpy as jnp
from jax import lax

D = 2048
HEAD = 64
A_HEADS = 16
A_KV = 4
MIXER_HEADS = 16
S_GROUPS = 4
STATE = 128
CONV = 5
WINDOW = 128
STATE_BLOCK = 128
TOK_DEV = 1024
SEQUENCE_LENGTH = 16384
S_INNER = 1024
N_TP = 2


def draw_inputs(key, part):
    base_key = jax.random.fold_in(key, 11)
    noise_key, row_key, column_key = jax.random.split(base_key, 3)
    row_scale = jnp.exp(jax.random.uniform(row_key, (SEQUENCE_LENGTH, 1), jnp.float32, 0.0, math.log(10.0)))
    column_ramp = jnp.exp(math.log(4.0) * jnp.arange(D, dtype=jnp.float32) / D)
    column_scale = column_ramp[None, :] * jnp.exp(jax.random.uniform(column_key, (1, D), jnp.float32, -0.5, 0.5))
    values = jnp.clip(jax.random.normal(noise_key, (SEQUENCE_LENGTH, D), jnp.float32), -4.0, 4.0)
    return (values * row_scale * column_scale).astype(jnp.bfloat16)


def gain_table(key, salt):
    gain_key = jax.random.fold_in(key, salt)
    return jax.random.uniform(gain_key, (HEAD,), jnp.float32, 0.5, 1.5)


def draw_query_gain(key, part):
    return gain_table(key, 21)


def draw_key_gain(key, part):
    return gain_table(key, 22)


def slow_heads(key):
    ranking = jax.random.permutation(jax.random.fold_in(key, 31), 2 * MIXER_HEADS)
    kept_count = MIXER_HEADS
    return (ranking < kept_count).reshape(2, MIXER_HEADS)


def base_rates(key):
    slowly = slow_heads(key)
    quick_rates = jax.random.uniform(jax.random.fold_in(key, 41), (2, MIXER_HEADS), jnp.float32, 1.5, 2.5) / STATE_BLOCK
    return jnp.where(slowly, 0.2 / SEQUENCE_LENGTH, quick_rates)


def draw_decay_rate(key, part):
    return base_rates(key)


def draw_decay_offset(key, part):
    rates = base_rates(key)
    device_blocks = SEQUENCE_LENGTH // TOK_DEV
    factor_key, position_random_key, level_random_key = jax.random.split(jax.random.fold_in(key, 51), 3)
    factors = jnp.exp(jax.random.uniform(factor_key, (device_blocks, 1, 2, MIXER_HEADS), jnp.float32, math.log(0.5), math.log(2.5)))
    constant_level = -jnp.broadcast_to(factors * rates, (device_blocks, TOK_DEV, 2, MIXER_HEADS)).reshape(SEQUENCE_LENGTH, 2, MIXER_HEADS)
    spike_position = jax.random.randint(position_random_key, (2, 2, MIXER_HEADS), 0, SEQUENCE_LENGTH)
    spike_level = jnp.log(jax.random.uniform(level_random_key, (2, 2, MIXER_HEADS), jnp.float32, 0.5, 0.8))
    spike_mask = jnp.arange(SEQUENCE_LENGTH)[:, None, None, None] == spike_position[None]
    spike_count = jnp.sum(jnp.where(spike_mask, spike_level[None], 0.0), axis=1)
    return constant_level + spike_count


def levels(key, extent, cuts, least, high):
    loudness, own = 1.0, jax.random.fold_in(key, 6)
    for dim, shards_of in cuts:
        draws = jnp.exp(jax.random.uniform(jax.random.fold_in(own, dim), (shards_of,), jnp.float32, least / len(cuts), high / len(cuts)))
        loudness = loudness * jnp.repeat(draws, extent[dim] // shards_of).reshape([-1 if axis == dim else 1 for axis in range(len(extent))])
    return loudness


def bell_draw(stream_key, extent, scale, reach, cuts=(), kind=jnp.bfloat16):
    result = jax.random.normal(stream_key, extent, jnp.float32) * scale
    if len(cuts) > 0:
        result = levels(stream_key, extent, cuts, -0.22, 0.18) * result
    return jnp.clip(result, min=-reach, max=reach).astype(kind)


def setup_inputs(seed: int = 0, part: int = 0) -> dict:
    splits = jax.random.split(jax.random.key(seed), 24)
    own_keys = jax.random.split(jax.random.fold_in(splits[23], part), 24)
    inputs = draw_inputs(jax.random.fold_in(jax.random.fold_in(splits[23], part), 71), part)
    mix_gain = jnp.clip(1.0 + 0.18 * jax.random.normal(splits[1], (D,), jnp.float32), 0.1, 1.9)
    w_query = bell_draw(splits[2], (D, A_HEADS * HEAD), D ** -0.5, 0.125, ((1, 2),))
    w_key = bell_draw(splits[3], (D, A_KV * HEAD), D ** -0.5, 0.125, ((1, 2),))
    w_value = bell_draw(splits[4], (D, A_KV * HEAD), D ** -0.5, 0.125, ((1, 2),))
    query_gain = draw_query_gain(jax.random.fold_in(splits[23], 71), part)
    key_gain = draw_key_gain(jax.random.fold_in(splits[23], 71), part)
    sink_logit = jnp.clip(3.0 + 4.0 * jax.random.uniform(splits[7], (A_HEADS,), jnp.float32) ** levels(splits[7], (A_HEADS,), ((0, 2),), -0.2, 0.2), 3.0, 7.0)
    w_inner = bell_draw(splits[8], (D, S_INNER), D ** -0.5, 0.125, ((1, 2),))
    w_bmat = bell_draw(splits[9], (D, S_GROUPS * STATE), D ** -0.5, 0.125, ((1, 2),))
    w_cmat = bell_draw(splits[10], (D, S_GROUPS * STATE), D ** -0.5, 0.125, ((1, 2),))
    w_gate = bell_draw(splits[11], (D, S_INNER), D ** -0.5, 0.125, ((1, 2),))
    w_step = bell_draw(splits[12], (D, 2, MIXER_HEADS), D ** -0.5, 0.125, ((2, 2),))
    conv_inner = bell_draw(splits[13], (CONV, S_INNER), CONV ** -0.5, 2.5, ((1, 2),))
    conv_bmat = bell_draw(splits[14], (CONV, S_GROUPS * STATE), CONV ** -0.5, 2.5, ((1, 2),))
    conv_cmat = bell_draw(splits[15], (CONV, S_GROUPS * STATE), CONV ** -0.5, 2.5, ((1, 2),))
    step_bias = jnp.clip(jax.random.uniform(splits[16], (2, MIXER_HEADS), jnp.float32, -1.0, 1.0) * levels(splits[16], (2, MIXER_HEADS), ((1, 2),), -0.4, 0.0), -1.0, 1.0)
    decay_rate = draw_decay_rate(jax.random.fold_in(splits[23], 71), part)
    decay_offset = draw_decay_offset(jax.random.fold_in(splits[23], 71), part)
    start_state = bell_draw(own_keys[19], (2, MIXER_HEADS, HEAD, STATE), (SEQUENCE_LENGTH ** 0.5 // 4), 192.0, ((1, 2),), jnp.float32)
    group_gain = jnp.clip(1.0 + 0.18 * jax.random.normal(splits[20], (S_INNER,), jnp.float32), 0.1, 1.9)
    w_out_attn = bell_draw(splits[21], (A_HEADS * HEAD, D), (A_HEADS * HEAD // 64) ** -0.5, 1.5, ((0, 2),))
    w_out_state = bell_draw(splits[22], (S_INNER, D), S_INNER ** -0.5, 0.1875, ((0, 2),))
    return dict(inputs=inputs, mix_gain=mix_gain, w_query=w_query, w_key=w_key, w_value=w_value, query_gain=query_gain, key_gain=key_gain, sink_logit=sink_logit, w_inner=w_inner, w_bmat=w_bmat, w_cmat=w_cmat, w_gate=w_gate, w_step=w_step, conv_inner=conv_inner, conv_bmat=conv_bmat, conv_cmat=conv_cmat, step_bias=step_bias, decay_rate=decay_rate, decay_offset=decay_offset, start_state=start_state, group_gain=group_gain, w_out_attn=w_out_attn, w_out_state=w_out_state)


epsilon = 1e-06
rotary_base = 10000.0

def head_norm(values, gain):
    return values * lax.rsqrt(lax.optimization_barrier(jnp.mean(values * values, axis=-1, keepdims=True)) + epsilon) * gain

def rotate(values, positions):
    half_dim = values.shape[-1] // 2
    frequency = rotary_base ** (-jnp.arange(half_dim, dtype=jnp.float32) / half_dim)
    angles = positions.astype(jnp.float32)[:, None] * frequency[None, :]
    shaped = (angles.shape[0],) + (1,) * (values.ndim - 2) + (half_dim,)
    cosine = jnp.cos(angles).reshape(shaped)
    sine_table = jnp.sin(angles).reshape(shaped)
    first_half = values[..., :half_dim]
    second_half = values[..., half_dim:]
    return jnp.concatenate([first_half * cosine - second_half * sine_table, second_half * cosine + first_half * sine_table], axis=-1)

def attend_block(queries, keys, values, sink_logit, key_pos, length):
    scores = jnp.einsum('qhgd,khd->hgqk', queries.astype(jnp.float32), keys.astype(jnp.float32)) * HEAD ** (-0.5)
    offsets = jnp.arange(3 * WINDOW) - WINDOW
    nearby = jnp.abs(offsets[None, :] - jnp.arange(WINDOW)[:, None]) <= WINDOW
    inside = (key_pos >= 0) & (key_pos < length)
    allowed = nearby & inside[None, :]
    masked = jnp.where(allowed, scores, -jnp.inf)
    highest = jnp.maximum(lax.optimization_barrier(jnp.max(masked, axis=-1, keepdims=True)), sink_logit[:, :, None, None])
    raised = jnp.exp(masked - highest)
    denominator = jnp.exp(sink_logit[:, :, None, None] - highest) + lax.optimization_barrier(jnp.sum(raised, axis=-1, keepdims=True))
    weights = (raised / denominator).astype(jnp.bfloat16)
    return jnp.einsum('hgqk,khe->qhge', weights.astype(jnp.float32), values.astype(jnp.float32)).astype(jnp.bfloat16)

def ssd_blocks(inner_act, bmat_act, cmat_act, step_size, log_decay, carry_state):
    length = inner_act.shape[0]
    number_blocks = length // STATE_BLOCK

    def split_blocks(values):
        return values.reshape((number_blocks, STATE_BLOCK) + values.shape[1:])
    causal = jnp.arange(STATE_BLOCK)[:, None] >= jnp.arange(STATE_BLOCK)[None, :]

    def advance(running, block_data):
        inner_rows, bmat_rows, cmat_rows, step_rows, decay_rows = block_data
        cumulative = jnp.cumsum(decay_rows, axis=0)
        scores = jnp.einsum('lgn,sgn->lsg', cmat_rows.astype(jnp.float32), bmat_rows.astype(jnp.float32))
        spread = jnp.where(causal[:, :, None, None], cumulative[:, None] - cumulative[None, :], -jnp.inf)
        weights = (scores[:, :, :, None] * jnp.exp(spread) * step_rows[None]).astype(jnp.bfloat16)
        within = jnp.einsum('lsgr,sgrp->lgrp', weights.astype(jnp.float32), inner_rows.astype(jnp.float32))
        carried = jnp.einsum('lgn,grpn->lgrp', cmat_rows.astype(jnp.float32), running, precision=lax.Precision.HIGHEST) * jnp.exp(cumulative)[..., None]
        fading = jnp.exp(cumulative[-1:] - cumulative)
        loaded = (inner_rows.astype(jnp.float32) * (step_rows * fading)[..., None]).astype(jnp.bfloat16)
        running = jnp.exp(cumulative[-1])[..., None, None] * running + jnp.einsum('sgrp,sgn->grpn', loaded.astype(jnp.float32), bmat_rows.astype(jnp.float32))
        return (running, within + carried)
    final_state, outputs = lax.scan(advance, carry_state, tuple((split_blocks(values) for values in (inner_act, bmat_act, cmat_act, step_size, log_decay))))
    return (final_state, outputs.reshape((length,) + outputs.shape[2:]))

def reverse_rows(values):
    return values[::-1]

def reference(inputs, mix_gain, w_query, w_key, w_value, query_gain, key_gain, sink_logit, w_inner, w_bmat, w_cmat, w_gate, w_step, conv_inner, conv_bmat, conv_cmat, step_bias, decay_rate, decay_offset, start_state, group_gain, w_out_attn, w_out_state):
    length = inputs.shape[0]
    widened = inputs.astype(jnp.float32)
    row_scale = lax.rsqrt(lax.optimization_barrier(jnp.mean(widened * widened, axis=1, keepdims=True)) + epsilon)
    scaled_in = (widened * mix_gain).astype(jnp.bfloat16)

    def project(weight):
        return row_scale * jnp.dot(scaled_in, weight, preferred_element_type=jnp.float32)
    query_proj = project(w_query).astype(jnp.bfloat16)
    key_proj = project(w_key).astype(jnp.bfloat16)
    value_proj = project(w_value).astype(jnp.bfloat16)
    inner_proj = project(w_inner).astype(jnp.bfloat16)
    bmat_proj = project(w_bmat).astype(jnp.bfloat16)
    cmat_proj = project(w_cmat).astype(jnp.bfloat16)
    gate_proj = project(w_gate).astype(jnp.bfloat16)
    step_raw = project(w_step.reshape(D, 2 * MIXER_HEADS)).reshape(length, 2, MIXER_HEADS)
    positions = jnp.arange(length, dtype=jnp.int32)
    group_size = A_HEADS // A_KV
    query_rot = rotate(head_norm(query_proj.astype(jnp.float32).reshape(length, A_HEADS, HEAD), query_gain), positions).astype(jnp.bfloat16).reshape(length, A_KV, group_size, HEAD)
    key_rot = rotate(head_norm(key_proj.astype(jnp.float32).reshape(length, A_KV, HEAD), key_gain), positions).astype(jnp.bfloat16)
    value_rows = value_proj.reshape(length, A_KV, HEAD)
    padding = ((WINDOW, WINDOW), (0, 0), (0, 0))
    key_padded = jnp.pad(key_rot, padding)
    value_padded = jnp.pad(value_rows, padding)
    sink_table = sink_logit.reshape(A_KV, group_size)

    def one_block(block_index):
        block_start = (block_index * WINDOW).astype(jnp.int32)
        query_block = lax.dynamic_slice_in_dim(query_rot, block_start, WINDOW, 0)
        key_block = lax.dynamic_slice_in_dim(key_padded, block_start, 3 * WINDOW, 0)
        value_block = lax.dynamic_slice_in_dim(value_padded, block_start, 3 * WINDOW, 0)
        key_pos = block_start - WINDOW + jnp.arange(3 * WINDOW, dtype=jnp.int32)
        return attend_block(query_block, key_block, value_block, sink_table, key_pos, length)
    attended = lax.map(one_block, jnp.arange(length // WINDOW, dtype=jnp.int32))
    attention_out = attended.reshape(length, A_HEADS * HEAD)
    mixed_rows = jnp.concatenate([inner_proj, bmat_proj, cmat_proj], axis=1)
    conv_taps = jnp.concatenate([conv_inner, conv_bmat, conv_cmat], axis=1).astype(jnp.float32)
    rim_width = CONV // 2
    framed = jnp.pad(mixed_rows, ((rim_width, rim_width), (0, 0))).astype(jnp.float32)
    conv_sum = jnp.zeros(mixed_rows.shape, jnp.float32)
    for tap_index in range(CONV):
        conv_sum = conv_sum + framed[tap_index:tap_index + length] * conv_taps[tap_index]
    activated = jax.nn.silu(conv_sum).astype(jnp.bfloat16)
    repeats = MIXER_HEADS // S_GROUPS
    state_width = S_GROUPS * STATE
    inner_act = activated[:, :S_INNER].reshape(length, S_GROUPS, repeats, HEAD)
    bmat_act = activated[:, S_INNER:S_INNER + state_width].reshape(length, S_GROUPS, STATE)
    cmat_act = activated[:, S_INNER + state_width:].reshape(length, S_GROUPS, STATE)
    step_size = jax.nn.softplus(step_raw + step_bias)
    log_decay = -decay_rate * step_size + decay_offset

    def shaped(values):
        return values.reshape(length, S_GROUPS, repeats)
    begin_fwd = start_state[0].reshape(S_GROUPS, repeats, HEAD, STATE)
    begin_bwd = start_state[1].reshape(S_GROUPS, repeats, HEAD, STATE)
    unused_fwd, output_fwd = ssd_blocks(inner_act, bmat_act, cmat_act, shaped(step_size[:, 0]), shaped(log_decay[:, 0]), begin_fwd)
    unused_bwd, output_bwd = ssd_blocks(reverse_rows(inner_act), reverse_rows(bmat_act), reverse_rows(cmat_act), reverse_rows(shaped(step_size[:, 1])), reverse_rows(shaped(log_decay[:, 1])), begin_bwd)
    state_sum = output_fwd + reverse_rows(output_bwd)
    group_width = repeats * HEAD
    gate_rows = gate_proj.astype(jnp.float32).reshape(length, S_GROUPS, group_width)
    gated = state_sum.reshape(length, S_GROUPS, group_width) * jax.nn.silu(gate_rows)
    normed = gated * lax.rsqrt(lax.optimization_barrier(jnp.mean(gated * gated, axis=-1, keepdims=True)) + epsilon)
    state_out = (normed * group_gain.reshape(S_GROUPS, group_width)).astype(jnp.bfloat16).reshape(length, S_INNER)
    attn_cols = A_HEADS * HEAD // N_TP
    state_cols = S_INNER // N_TP
    summed = jnp.zeros((length, D), jnp.float32)
    for part_index in range(N_TP):
        partial_value = jnp.dot(attention_out[:, part_index * attn_cols:(part_index + 1) * attn_cols], w_out_attn[part_index * attn_cols:(part_index + 1) * attn_cols], preferred_element_type=jnp.float32)
        partial_value = partial_value + jnp.dot(state_out[:, part_index * state_cols:(part_index + 1) * state_cols], w_out_state[part_index * state_cols:(part_index + 1) * state_cols], preferred_element_type=jnp.float32)
        summed = summed + lax.optimization_barrier(partial_value.astype(jnp.bfloat16)).astype(jnp.float32)
    return summed.astype(jnp.bfloat16)
```

```python
import functools

import jax
import jax.numpy as jnp
import numpy as np
from jax import lax
from jax.experimental import pallas as pl
from jax.experimental.pallas import tpu as pltpu
from jax.sharding import PartitionSpec as P

D = 2048
HALF = 1024
HEAD = 64
STATE = 128
CONV = 5
BLOCK = 128
EPS = 1e-06
BASE = 10000.0
HEADS = 8
ROWS = 512
f32 = jnp.float32
bf16 = jnp.bfloat16


def dot(a, b):
    return jnp.dot(a, b, preferred_element_type=f32)


def dot_rt(a, b):
    return lax.dot_general(a, b, (((1,), (1,)), ((), ())), preferred_element_type=f32)


def split2(v):
    hi = v.astype(bf16).astype(f32)
    return hi, (v - hi).astype(bf16).astype(f32)


def split3(v):
    hi = v.astype(bf16).astype(f32)
    rest = v - hi
    mid = rest.astype(bf16).astype(f32)
    return hi, mid, (rest - mid).astype(bf16).astype(f32)


def iota(shape, dim):
    return lax.broadcasted_iota(jnp.int32, shape, dim)


def whole(shape):
    zeros = (0,) * len(shape)
    return pl.BlockSpec(shape, lambda *_: zeros)


def once(shape):
    zeros = (0,) * len(shape)
    return pl.BlockSpec(shape, lambda *_: zeros, pipeline_mode=pl.Buffered(1))


def sds(shape, dtype):
    return jax.ShapeDtypeStruct(shape, dtype)


def rotation_tables(positions):
    lane = np.arange(128) % 32
    freq = BASE ** (-lane.astype(np.float64) / 32)
    angles = positions.astype(np.float64)[:, None] * freq[None, :]
    return np.cos(angles).astype(np.float32), np.sin(angles).astype(np.float32)


def project_kernel(
    ids, xo, xp, gain, wq, wk, wv, wi, wb, wc, ws, qg, kg, cosb, sinb, cosi, sini,
    q_o, kv_o, p1_o, st_o, xs_o, rs_o, lo_o, hi_o,
):
    i = pl.program_id(0)
    t = ids[0]
    sp = ids[1]
    own = pl.multiple_of(t * HALF, HALF)
    peer = pl.multiple_of((1 - t) * HALF, HALF)
    own_x = xo[...].astype(f32)
    peer_x = xp[...].astype(f32)
    squares = jnp.sum(own_x * own_x, axis=1, keepdims=True) + jnp.sum(
        peer_x * peer_x, axis=1, keepdims=True
    )
    rs = lax.rsqrt(squares * (1.0 / D) + EPS)
    rs_o[...] = jnp.broadcast_to(rs, (ROWS, 128))
    xs_o[:, pl.ds(own, HALF)] = (own_x * gain[:, pl.ds(own, HALF)]).astype(bf16)
    xs_o[:, pl.ds(peer, HALF)] = (peer_x * gain[:, pl.ds(peer, HALF)]).astype(bf16)

    def proj(w):
        return dot(xs_o[...], w[...]) * rs

    p1_o[:, 0:512] = proj(wi).astype(bf16)
    p1_o[:, 512:768] = proj(wb).astype(bf16)
    p1_o[:, 768:1024] = proj(wc).astype(bf16)
    st_o[...] = proj(ws).T[0:16, :]

    lane = iota((1, 128), 1)
    first = (lane % HEAD) < (HEAD // 2)
    cosines, sines = [], []
    for s in range(ROWS // BLOCK):
        index = sp * 8 + i * (ROWS // BLOCK) + s
        cb = cosb[pl.ds(index, 1), :]
        sb = sinb[pl.ds(index, 1), :]
        cosines.append(cb * cosi[...] - sb * sini[...])
        sine = sb * cosi[...] + cb * sini[...]
        sines.append(jnp.where(first, -sine, sine))
    cosine = jnp.concatenate(cosines, axis=0)
    sine = jnp.concatenate(sines, axis=0)
    same = (iota((128, 128), 0) // HEAD) == (iota((128, 128), 1) // HEAD)
    averaging = jnp.where(same, 1.0 / HEAD, 0.0).astype(bf16)

    def normed_rotated(values, head_gain):
        values = values.astype(bf16).astype(f32)
        hi, lo = split2(values * values)
        mean = dot(hi.astype(bf16), averaging) + dot(lo.astype(bf16), averaging)
        y = values * lax.rsqrt(mean + EPS) * head_gain
        swapped = jnp.where(first, pltpu.roll(y, 96, 1), pltpu.roll(y, 32, 1))
        return (y * cosine + swapped * sine).astype(bf16)

    queries = proj(wq)
    for j in range(4):
        q_o[:, 128 * j : 128 * (j + 1)] = normed_rotated(
            queries[:, 128 * j : 128 * (j + 1)], qg[...]
        )
    kv_o[:, 0:128] = normed_rotated(proj(wk), kg[...])
    kv_o[:, 128:256] = proj(wv).astype(bf16)

    @pl.when(i == 0)
    def _():
        lo_o[0:128, :] = kv_o[0:128, :]
        for j in range(4):
            lo_o[128 + 16 * j : 144 + 16 * j, :] = p1_o[0:16, 256 * j : 256 * (j + 1)]

    @pl.when(i == pl.num_programs(0) - 1)
    def _():
        hi_o[0:128, :] = kv_o[ROWS - 128 : ROWS, :]
        for j in range(4):
            hi_o[128 + 16 * j : 144 + 16 * j, :] = p1_o[
                ROWS - 16 : ROWS, 256 * j : 256 * (j + 1)
            ]


def gate_kernel(xs, rs, wg, st, bias, rate, offset, gate_o, rows_o, col_o):
    gate_o[...] = (dot(xs[...], wg[...]) * rs[:, 0:1]).astype(bf16)
    v = st[...] + bias[:, 0:1]
    step = jnp.maximum(v, 0.0) + jnp.log1p(jnp.exp(-jnp.abs(v)))
    decay = -rate[:, 0:1] * step + offset[...]
    count = ROWS // BLOCK
    parts = [decay[:, BLOCK * s : BLOCK * (s + 1)] for s in range(count)]
    stacked = jnp.concatenate(parts, axis=0)
    hi, mid, lo = split3(stacked)
    row = iota((128, 256), 0)
    column = iota((128, 256), 1)
    prefix = (column < 128) & (row <= column)
    suffix = (column >= 128) & (row >= column - 128)
    sums = jnp.where(prefix | suffix, 1.0, 0.0).astype(bf16)
    total = dot(hi.astype(bf16), sums) + dot(mid.astype(bf16), sums) + dot(lo.astype(bf16), sums)
    for s in range(count):
        c = jnp.concatenate(
            [total[16 * s : 16 * s + 8, 0:128], total[16 * s + 8 : 16 * s + 16, 128:256]], axis=0
        )
        steps = step[:, BLOCK * s : BLOCK * (s + 1)]
        last = jnp.concatenate([c[0:8, 127:128], c[8:16, 0:1]], axis=0)
        factor = steps * jnp.exp(last - c)
        raised = jnp.exp(c)
        rows_o[s, 0:16, :] = jnp.log(steps) - c
        rows_o[s, 16:24, :] = steps[0:8] + steps[8:16]
        factor_hi, factor_lo = split2(factor)
        raised_hi, raised_lo = split2(raised)
        packed = jnp.concatenate(
            [c, factor_hi, factor_lo, raised_hi, raised_lo, jnp.zeros((48, 128), f32)], axis=0
        )
        col_o[BLOCK * s : BLOCK * (s + 1), :] = packed.T


def mixer_kernel(
    p1, lo, hi, taps, rows, col, expand, pick,
    within_o, cmat_o, add_o, tot_o, pack_o,
    xpad, run_f, run_b, prod_f, prod_b,
):
    b = pl.program_id(0)
    start = pl.multiple_of(b * BLOCK, BLOCK)

    @pl.when(b == 0)
    def _():
        run_f[...] = jnp.zeros_like(run_f)
        run_b[...] = jnp.zeros_like(run_b)
        prod_f[...] = jnp.ones_like(prod_f)
        prod_b[...] = jnp.ones_like(prod_b)
        for j in range(4):
            xpad[0:8, 256 * j : 256 * (j + 1)] = lo[128 + 16 * j : 144 + 16 * j, :].astype(f32)[
                8:16
            ]

    @pl.when(b > 0)
    def _():
        before = pl.multiple_of(jnp.maximum(start - 16, 0), 16)
        xpad[0:8, :] = p1[pl.ds(before, 16), :].astype(f32)[8:16]

    @pl.when(b < 7)
    def _():
        after = pl.multiple_of(jnp.minimum(start + BLOCK, 1008), 16)
        xpad[136:144, :] = p1[pl.ds(after, 16), :].astype(f32)[0:8]

    @pl.when(b == 7)
    def _():
        for j in range(4):
            xpad[136:144, 256 * j : 256 * (j + 1)] = hi[128 + 16 * j : 144 + 16 * j, :].astype(
                f32
            )[0:8]

    xpad[8:136, :] = p1[pl.ds(start, BLOCK), :].astype(f32)

    def convolved(low, high):
        total = taps[0:1, low:high] * xpad[6:134, low:high]
        for j in range(1, CONV):
            total = total + taps[j : j + 1, low:high] * xpad[6 + j : 134 + j, low:high]
        return (total / (1.0 + jnp.exp(-total))).astype(bf16)

    inner = convolved(0, 512)
    bmat = convolved(512, 768)
    cmat = convolved(768, 1024)
    cmat_o[...] = cmat
    c_col = col[...]
    widened = dot(c_col.astype(bf16), expand[...])
    inner_wide = inner.astype(f32)
    loaded_f = (inner_wide * widened[:, 0:512]).astype(bf16)
    loaded_b = (inner_wide * widened[:, 512:1024]).astype(bf16)
    tot_f = widened[127:128, 1024:1536]
    tot_b = widened[0:1, 1536:2048]
    tot_o[pl.ds(b, 1), 0:512] = tot_f
    tot_o[pl.ds(b, 1), 512:1024] = tot_b
    row = iota((128, 128), 0)
    column = iota((128, 128), 1)
    causal = row >= column
    diagonal = row == column
    low_lane = iota((1, 128), 1) < HEAD
    for g in range(2):
        bg = bmat[:, 128 * g : 128 * (g + 1)]
        cg = cmat[:, 128 * g : 128 * (g + 1)]
        scores = dot_rt(cg, bg)
        flipped = bg.astype(f32).T.astype(bf16)
        cols = slice(256 * g, 256 * (g + 1))
        add_f = dot(flipped, loaded_f[:, cols])
        add_b = dot(flipped, loaded_b[:, cols])
        add_o[0, 0, :, cols] = add_f
        add_o[0, 1, :, cols] = add_b
        run_f[:, cols] = tot_f[:, cols] * run_f[:, cols] + add_f
        run_b[:, cols] = run_b[:, cols] + prod_b[:, cols] * add_b
        for pair in range(2):
            weights = []
            for r in range(2):
                h = 4 * g + 2 * pair + r
                forward = c_col[:, h : h + 1] + rows[0, h : h + 1, :]
                backward = c_col[:, 8 + h : 9 + h] + rows[0, 8 + h : 9 + h, :]
                spread = jnp.exp(jnp.where(causal, forward, backward))
                spread = jnp.where(diagonal, rows[0, 16 + h : 17 + h, :], spread)
                weights.append((scores * spread).astype(bf16))
            base = 256 * g + 128 * pair
            both = inner[:, base : base + 128]
            zero = jnp.zeros_like(both)
            right = jnp.concatenate(
                [jnp.where(low_lane, both, zero), jnp.where(low_lane, zero, both)], axis=0
            )
            within_o[:, base : base + 128] = dot(jnp.concatenate(weights, axis=1), right)
    prod_f[...] = prod_f[...] * tot_f
    prod_b[...] = prod_b[...] * tot_b

    @pl.when(b == 7)
    def _():
        levels = jnp.concatenate([prod_f[...], prod_b[...]], axis=0)
        hi_l, mid_l, lo_l = split3(levels)
        joined = jnp.concatenate([hi_l, mid_l, lo_l], axis=1).astype(bf16)
        sent = dot(joined, pick[...])
        sent = jnp.concatenate(
            [jnp.broadcast_to(sent[0:1], (8, 128)), jnp.broadcast_to(sent[1:2], (8, 128))], axis=0
        ).astype(bf16)
        for j in range(16):
            pack_o[j, :, 0:512] = jnp.concatenate(
                [run_f[8 * j : 8 * j + 8, :], run_b[8 * j : 8 * j + 8, :]], axis=0
            ).astype(bf16)
            pack_o[j, :, 512:640] = sent


def carry_kernel(ids, arrived, start, spread, out, wide, held):
    for j in range(16):
        wide[j] = dot(arrived[j, :, 512:640], spread[...])
    state = start[0, 0]
    for j in range(16):
        held[j, 0:8, :] = state
        state = wide[j, 0:8, :] * state + arrived[j, :, 0:512].astype(f32)[0:8]
    state = start[1, 0]
    for j in reversed(range(16)):
        held[j, 8:16, :] = state
        state = wide[j, 8:16, :] * state + arrived[j, :, 0:512].astype(f32)[8:16]
    for j in range(16):
        out[j] = held[j].astype(bf16)


def enter_kernel(arrived, add, tot, out):
    state = jnp.concatenate([arrived[j].astype(f32)[0:8] for j in range(16)], axis=0)
    for b in range(8):
        out[b, :, 0:512] = state.astype(bf16)
        if b < 7:
            state = tot[b : b + 1, 0:512] * state + add[b, 0]
    state = jnp.concatenate([arrived[j].astype(f32)[8:16] for j in range(16)], axis=0)
    for b in reversed(range(8)):
        out[b, :, 512:1024] = state.astype(bf16)
        if b > 0:
            state = tot[b : b + 1, 512:1024] * state + add[b, 1]


def attend_kernel(ids, q, kv, lo, hi, sink, out, keys, vals):
    b = pl.program_id(0)
    sp = ids[1]
    low_lane = iota((1, 128), 1) < HEAD

    def place(first, count, kk, vv):
        kk = kk.astype(f32)
        vv = vv.astype(f32)
        kr = pltpu.roll(kk, 64, 1)
        vr = pltpu.roll(vv, 64, 1)
        span = slice(first, first + count)
        keys[0, span, :] = jnp.where(low_lane, kk, kr).astype(bf16)
        keys[1, span, :] = jnp.where(low_lane, kr, kk).astype(bf16)
        vals[0, span, :] = jnp.where(low_lane, vv, 1.0).astype(bf16)
        vals[1, span, :] = jnp.where(low_lane, 1.0, vr).astype(bf16)
        vals[2, span, :] = jnp.where(low_lane, vr, 1.0).astype(bf16)
        vals[3, span, :] = jnp.where(low_lane, 1.0, vv).astype(bf16)

    @pl.when(b == 0)
    def _():
        place(0, 128, lo[0:128, 0:128], lo[0:128, 128:256])
        place(128, 1024, kv[:, 0:128], kv[:, 128:256])
        place(1152, 128, hi[0:128, 0:128], hi[0:128, 128:256])

    start = pl.multiple_of(b * BLOCK, BLOCK)
    row = iota((128, 384), 0)
    column = iota((128, 384), 1)
    least = jnp.where((b == 0) & (sp == 0), 128, 0)
    limit = jnp.where((b == 7) & (sp == 15), 256, 384)
    allowed = (column >= row) & (column <= row + 256) & (column >= least) & (column < limit)
    bias = jnp.where(allowed, 0.0, -1e30)
    bias = jnp.concatenate([bias, bias], axis=0)
    for g in range(2):
        kg = keys[g, pl.ds(start, 384), :]
        tiles = [
            (q[:, 256 * g + 128 * j : 256 * g + 128 * (j + 1)].astype(f32) * 0.125).astype(bf16)
            for j in range(2)
        ]
        results, sinks = [], []
        for parity in range(2):
            keep = low_lane if parity == 0 else jnp.logical_not(low_lane)
            stacked = jnp.concatenate(
                [jnp.where(keep, tile, jnp.zeros_like(tile)) for tile in tiles], axis=0
            )
            scores = dot_rt(stacked, kg) + bias
            first_sink = sink[4 * g + parity : 4 * g + parity + 1, 0:1]
            second_sink = sink[4 * g + 2 + parity : 4 * g + 3 + parity, 0:1]
            sink_col = jnp.concatenate(
                [jnp.broadcast_to(first_sink, (128, 1)), jnp.broadcast_to(second_sink, (128, 1))],
                axis=0,
            )
            highest = jnp.maximum(jnp.max(scores, axis=1, keepdims=True), sink_col)
            weights = jnp.exp(scores - highest).astype(bf16)
            results.append(dot(weights, vals[2 * g + parity, pl.ds(start, 384), :]))
            sinks.append(jnp.exp(sink_col - highest))
        numerator = jnp.where(low_lane, results[0], results[1])
        other = jnp.where(low_lane, results[1], results[0])
        denominator = pltpu.roll(other, 64, 1) + jnp.where(low_lane, sinks[0], sinks[1])
        final = (numerator / denominator).astype(bf16)
        out[:, 256 * g : 256 * g + 128] = final[0:128]
        out[:, 256 * g + 128 : 256 * g + 256] = final[128:256]


def output_kernel(ids, attn, within, cmat, gate, col, entering, expand, gain, wa, ws, out, mixed):
    @pl.when(pl.program_id(0) == 0)
    def _():
        for s in range(ROWS // BLOCK):
            span = slice(BLOCK * s, BLOCK * (s + 1))
            widened = dot(col[span, :].astype(bf16), expand[:, 1024:2048])
            for g in range(2):
                cg = cmat[span, 128 * g : 128 * (g + 1)]
                cols = slice(256 * g, 256 * (g + 1))
                cols_b = slice(512 + 256 * g, 512 + 256 * (g + 1))
                total = within[span, cols]
                total = total + widened[:, cols] * dot(cg, entering[s, :, cols])
                total = total + widened[:, cols_b] * dot(cg, entering[s, :, cols_b])
                gates = gate[span, cols].astype(f32)
                gated = total * (gates / (1.0 + jnp.exp(-gates)))
                mean = jnp.mean(gated * gated, axis=1, keepdims=True)
                mixed[span, cols] = (
                    gated * lax.rsqrt(mean + EPS) * gain[:, cols]
                ).astype(bf16)

    out[...] = (dot(attn[...], wa[...]) + dot(mixed[...], ws[...])).astype(bf16)


def call(kernel, name, grid, in_specs, out_specs, out_shape, scratch=(), scalars=0, flops=0, nbytes=0):
    return pl.pallas_call(
        kernel,
        name=name,
        grid_spec=pltpu.PrefetchScalarGridSpec(
            num_scalar_prefetch=scalars,
            grid=grid,
            in_specs=in_specs,
            out_specs=out_specs,
            scratch_shapes=list(scratch),
        ),
        out_shape=out_shape,
        cost_estimate=pl.CostEstimate(flops=flops, transcendentals=0, bytes_accessed=nbytes),
        compiler_params=pltpu.CompilerParams(
            dimension_semantics=("arbitrary",) * len(grid), vmem_limit_bytes=60000 * 1024
        ),
    )


def local(
    inputs, mix_gain, w_query, w_key, w_value, query_gain, key_gain, sink_logit, w_inner, w_bmat,
    w_cmat, w_gate, w_step, conv_inner, conv_bmat, conv_cmat, step_bias, decay_rate, decay_offset,
    start_state, group_gain, w_out_attn, w_out_state,
):
    sp_count = lax.axis_size("sp")
    tp = lax.axis_index("tp")
    sp = lax.axis_index("sp")
    ids = jnp.stack([tp, sp, jnp.zeros_like(tp)]).astype(jnp.int32)
    swap = [(0, 1), (1, 0)]
    other = lax.ppermute(inputs, "tp", swap)

    cosb, sinb = rotation_tables(np.arange(128) * BLOCK)
    cosi, sini = rotation_tables(np.arange(BLOCK))
    step_w = jnp.pad(w_step.reshape(D, 16), ((0, 0), (0, 112)))
    tile_gain = lambda gain: jnp.tile(gain, 2).reshape(1, 128)
    rows2 = lambda width: pl.BlockSpec((ROWS, width), lambda i, *_: (i, 0))
    grid = (1024 // ROWS,)
    q_rot, kv, p1, step_t, xs, rs, lo_edge, hi_edge = call(
        project_kernel, "project", grid,
        [
            rows2(HALF), rows2(HALF), once((1, D)), once((D, 512)), once((D, 128)), once((D, 128)),
            once((D, 512)), once((D, 256)), once((D, 256)), once((D, 128)), once((1, 128)),
            once((1, 128)), once((128, 128)), once((128, 128)), once((128, 128)), once((128, 128)),
        ],
        [
            rows2(512), rows2(256), rows2(1024), pl.BlockSpec((16, ROWS), lambda i, *_: (0, i)),
            rows2(D), rows2(128), whole((192, 256)), whole((192, 256)),
        ],
        [
            sds((1024, 512), bf16), sds((1024, 256), bf16), sds((1024, 1024), bf16),
            sds((16, 1024), f32), sds((1024, D), bf16), sds((1024, 128), f32),
            sds((192, 256), bf16), sds((192, 256), bf16),
        ],
        scalars=1, flops=2 * 1024 * D * 1808, nbytes=20 << 20,
    )(
        ids, inputs, other, mix_gain.reshape(1, D), w_query, w_key, w_value, w_inner, w_bmat,
        w_cmat, step_w, tile_gain(query_gain), tile_gain(key_gain), cosb, sinb, cosi, sini,
    )

    forward = [(i, i + 1) for i in range(sp_count - 1)]
    backward = [(i + 1, i) for i in range(sp_count - 1)]
    lo = lax.ppermute(hi_edge, "sp", forward)
    hi = lax.ppermute(lo_edge, "sp", backward)

    column = lambda value: jnp.broadcast_to(value.reshape(16, 1), (16, 128))
    offset_t = decay_offset.reshape(1024, 16).T
    gate, rows, col = call(
        gate_kernel, "gate", grid,
        [
            rows2(D), rows2(128), once((D, 512)), pl.BlockSpec((16, ROWS), lambda i: (0, i)),
            once((16, 128)), once((16, 128)), pl.BlockSpec((16, ROWS), lambda i: (0, i)),
        ],
        [rows2(512), pl.BlockSpec((ROWS // BLOCK, 24, 128), lambda i: (i, 0, 0)), rows2(128)],
        [sds((1024, 512), bf16), sds((8, 24, 128), f32), sds((1024, 128), f32)],
        flops=2 * 1024 * D * 512, nbytes=8 << 20,
    )(xs, rs, w_gate, step_t, column(step_bias), column(decay_rate), offset_t)

    lane = np.arange(1024)
    unit = lane // HEAD
    expand = np.zeros((128, 2048), np.float32)
    for u in range(16):
        for base, shift in ((16, 0), (32, 0), (48, 1024), (64, 1024)):
            expand[base + u, shift : shift + 1024] = unit == u
    expand = jnp.asarray(expand, bf16)
    pick = np.zeros((1536, 128), np.float32)
    for part in range(3):
        for h in range(HEADS):
            pick[512 * part + HEAD * h, 8 * part + h] = 1
    pick = jnp.asarray(pick, bf16)
    spread = np.zeros((128, 512), np.float32)
    for j in range(24):
        spread[j] = (lane[:512] // HEAD) == (j % 8)
    spread = jnp.asarray(spread, bf16)
    taps = jnp.concatenate([conv_inner, conv_bmat, conv_cmat], axis=1).astype(f32)

    rows1 = lambda width: pl.BlockSpec((BLOCK, width), lambda b, *_: (b, 0))
    within, cmat, add, tot, pack = call(
        mixer_kernel, "mixer", (8,),
        [
            once((1024, 1024)), once((192, 256)), once((192, 256)), once((CONV, 1024)),
            pl.BlockSpec((1, 24, 128), lambda b: (b, 0, 0)), rows1(128), once((128, 2048)),
            once((1536, 128)),
        ],
        [
            rows1(512), rows1(256), pl.BlockSpec((1, 2, 128, 512), lambda b: (b, 0, 0, 0)),
            whole((8, 1024)), whole((16, 16, 640)),
        ],
        [
            sds((1024, 512), f32), sds((1024, 256), bf16), sds((8, 2, 128, 512), f32),
            sds((8, 1024), f32), sds((16, 16, 640), bf16),
        ],
        scratch=[
            pltpu.VMEM((144, 1024), f32), pltpu.VMEM((128, 512), f32), pltpu.VMEM((128, 512), f32),
            pltpu.VMEM((1, 512), f32), pltpu.VMEM((1, 512), f32),
        ],
        flops=1 << 30, nbytes=12 << 20,
    )(p1, lo, hi, taps, rows, col, expand, pick)

    arrived = lax.all_to_all(pack, "sp", 0, 0, tiled=True)
    start_t = start_state.reshape(2, 512, 16, 8).transpose(0, 2, 3, 1)
    carried = call(
        carry_kernel, "carry", (1,),
        [
            whole((16, 16, 640)),
            pl.BlockSpec((2, 1, 8, 512), lambda i, ids: (0, ids[1], 0, 0)), whole((128, 512)),
        ],
        whole((16, 16, 512)), sds((16, 16, 512), bf16),
        scratch=[pltpu.VMEM((16, 16, 512), f32), pltpu.VMEM((16, 16, 512), f32)],
        scalars=1, flops=1 << 22, nbytes=1 << 20,
    )(ids, arrived, start_t, spread)
    returned = lax.all_to_all(carried, "sp", 0, 0, tiled=True)

    sink = jnp.broadcast_to(sink_logit.reshape(HEADS, 1), (HEADS, 128))
    attention = call(
        attend_kernel, "attend", (8,),
        [rows1(512), once((1024, 256)), once((192, 256)), once((192, 256)), once((HEADS, 128))],
        rows1(512), sds((1024, 512), bf16),
        scratch=[pltpu.VMEM((2, 1280, 128), bf16), pltpu.VMEM((4, 1280, 128), bf16)],
        scalars=1, flops=1 << 31, nbytes=4 << 20,
    )(ids, q_rot, kv, lo, hi, sink)

    entering = call(
        enter_kernel, "enter", (1,),
        [whole((16, 16, 512)), whole((8, 2, 128, 512)), whole((8, 1024))],
        whole((8, 128, 1024)), sds((8, 128, 1024), bf16), flops=1 << 22, nbytes=6 << 20,
    )(returned, add, tot)

    def projected(half):
        rows_half = lambda width: pl.BlockSpec((ROWS, width), lambda n, ids: (ids[0], 0))
        weight = pl.BlockSpec((512, 512), lambda n, ids: (0, n))
        return call(
            output_kernel, "output", (4,),
            [
                rows_half(512), rows_half(512), rows_half(256), rows_half(512), rows_half(128),
                pl.BlockSpec((4, 128, 1024), lambda n, ids: (ids[0], 0, 0)), once((128, 2048)),
                once((1, 512)), weight, weight,
            ],
            pl.BlockSpec((ROWS, 512), lambda n, ids: (0, n)), sds((ROWS, D), bf16),
            scratch=[pltpu.VMEM((ROWS, 512), bf16)], scalars=1, flops=2 * 512 * 1024 * D,
            nbytes=8 << 20,
        )(
            half.reshape(1).astype(jnp.int32), attention, within, cmat, gate, col, entering,
            expand, group_gain.reshape(1, 512), w_out_attn, w_out_state,
        )

    sent = projected(1 - tp)
    received = lax.ppermute(sent, "tp", swap)
    kept = projected(tp)
    return (kept.astype(f32) + received.astype(f32)).astype(bf16)


def solution(mesh):
    return jax.shard_map(
        local,
        mesh=mesh,
        in_specs=(
            P(("fs", "sp"), "tp"), P(), P(None, "tp"), P(None, "tp"), P(None, "tp"), P(), P(),
            P("tp"), P(None, "tp"), P(None, "tp"), P(None, "tp"), P(None, "tp"),
            P(None, None, "tp"), P(None, "tp"), P(None, "tp"), P(None, "tp"), P(None, "tp"),
            P(None, "tp"), P("sp", None, "tp"), P("fs", "tp", None, None), P("tp"),
            P("tp", None), P("tp", None),
        ),
        out_specs=P(("fs", "sp", "tp"), None),
        check_vma=False,
    )
```

```python
import functools

import jax
import jax.numpy as jnp
import numpy as np
from jax import lax
from jax.experimental import pallas as pl
from jax.experimental.pallas import tpu as pltpu
from jax.sharding import PartitionSpec as P

D = 2048
HALF = 1024
HEAD = 64
STATE = 128
CONV = 5
BLOCK = 128
EPS = 1e-06
BASE = 10000.0
HEADS = 8
ROWS = 512
SPAN = 256
f32 = jnp.float32
bf16 = jnp.bfloat16


def dot(a, b):
    return jnp.dot(a, b, preferred_element_type=f32)


def dot_rt(a, b):
    return lax.dot_general(a, b, (((1,), (1,)), ((), ())), preferred_element_type=f32)


def split2(v):
    hi = v.astype(bf16).astype(f32)
    return hi, (v - hi).astype(bf16).astype(f32)


def split3(v):
    hi = v.astype(bf16).astype(f32)
    rest = v - hi
    mid = rest.astype(bf16).astype(f32)
    return hi, mid, (rest - mid).astype(bf16).astype(f32)


def iota(shape, dim):
    return lax.broadcasted_iota(jnp.int32, shape, dim)


def whole(shape):
    zeros = (0,) * len(shape)
    return pl.BlockSpec(shape, lambda *_: zeros)


def once(shape):
    zeros = (0,) * len(shape)
    return pl.BlockSpec(shape, lambda *_: zeros, pipeline_mode=pl.Buffered(1))


def near(value):
    return pltpu.with_memory_space_constraint(value, pltpu.VMEM)


def far(value):
    return pltpu.with_memory_space_constraint(value, pltpu.HBM)


VM = pl.BlockSpec(memory_space=pltpu.VMEM)


def hbm(shape, dtype):
    return pltpu.HBM(shape, dtype)


def sds(shape, dtype):
    return jax.ShapeDtypeStruct(shape, dtype)


def rotation_tables(positions):
    lane = np.arange(128) % 32
    freq = BASE ** (-lane.astype(np.float64) / 32)
    angles = positions.astype(np.float64)[:, None] * freq[None, :]
    return np.cos(angles).astype(np.float32), np.sin(angles).astype(np.float32)


def project_kernel(
    xo, xp, gain, wq, wk, wv, wi, wb, wc, ws, qg, kg, cosb, sinb, cosi, sini,
    q_o, kv_o, p1_o, st_o, xs_o, rs_o, lo_o, hi_o, wkv, means, scaled,
):
    i = pl.program_id(0)
    t = lax.axis_index("tp")
    sp = lax.axis_index("sp")
    own = pl.multiple_of(t * HALF, HALF)
    peer = pl.multiple_of((1 - t) * HALF, HALF)

    @pl.when(i == 0)
    def _():
        wkv[:, 0:128] = wk[...]
        wkv[:, 128:256] = wv[...]

    own_x = xo[...].astype(f32)
    peer_x = xp[pl.ds(pl.multiple_of(i * ROWS, ROWS), ROWS), :].astype(f32)
    xs_o[:, pl.ds(own, HALF)] = (own_x * gain[:, pl.ds(own, HALF)]).astype(bf16)
    xs_o[:, pl.ds(peer, HALF)] = (peer_x * gain[:, pl.ds(peer, HALF)]).astype(bf16)
    squares = jnp.sum(own_x * own_x, axis=1, keepdims=True) + jnp.sum(
        peer_x * peer_x, axis=1, keepdims=True
    )
    rs = lax.rsqrt(squares * (1.0 / D) + EPS)
    rs_o[...] = jnp.broadcast_to(rs, (ROWS, 128))

    def proj(w):
        return dot(xs_o[...], w[...]) * rs

    q_o[...] = proj(wq).astype(bf16)
    kv_o[...] = proj(wkv).astype(bf16)
    tiles = [q_o.at[:, 128 * j : 128 * (j + 1)] for j in range(4)] + [kv_o.at[:, 0:128]]
    same = (iota((128, 128), 0) // HEAD) == (iota((128, 128), 1) // HEAD)
    averaging = jnp.where(same, 1.0 / HEAD, 0.0).astype(bf16)
    for j, tile in enumerate(tiles):
        values = tile[...].astype(f32)
        hi, lo = split2(values * values)
        scaled[0, j] = hi.astype(bf16)
        scaled[1, j] = lo.astype(bf16)
    for j in range(5):
        means[j] = dot(scaled[0, j], averaging) + dot(scaled[1, j], averaging)
    p1_o[:, 0:512] = proj(wi).astype(bf16)
    lane = iota((1, 128), 1)
    first = (lane % HEAD) < (HEAD // 2)
    query_gain = jnp.concatenate([qg[...], qg[...]], axis=1)
    key_gain = jnp.concatenate([kg[...], kg[...]], axis=1)
    for s in range(ROWS // BLOCK):
        span = slice(BLOCK * s, BLOCK * (s + 1))
        index = sp * 8 + i * (ROWS // BLOCK) + s
        cb = cosb[pl.ds(index, 1), :]
        sb = sinb[pl.ds(index, 1), :]
        cosine = cb * cosi[...] - sb * sini[...]
        sine = sb * cosi[...] + cb * sini[...]
        sine = jnp.where(first, -sine, sine)
        for j, tile in enumerate(tiles):
            head_gain = query_gain if j < 4 else key_gain
            y = tile[span, :].astype(f32) * lax.rsqrt(means[j, span, :] + EPS) * head_gain
            swapped = jnp.where(first, pltpu.roll(y, 96, 1), pltpu.roll(y, 32, 1))
            tile[span, :] = (y * cosine + swapped * sine).astype(bf16)
    p1_o[:, 512:768] = proj(wb).astype(bf16)
    p1_o[:, 768:1024] = proj(wc).astype(bf16)
    steps = dot_rt(xs_o[...], ws[...]) * rs
    st_o[...] = jnp.concatenate([steps, jnp.zeros((ROWS, 112), f32)], axis=1).T[0:16, :]

    @pl.when(i == 0)
    def _():
        lo_o[0:128, :] = kv_o[0:128, :]
        for j in range(4):
            lo_o[128 + 16 * j : 144 + 16 * j, :] = p1_o[0:16, 256 * j : 256 * (j + 1)]

    @pl.when(i == pl.num_programs(0) - 1)
    def _():
        hi_o[0:128, :] = kv_o[ROWS - 128 : ROWS, :]
        for j in range(4):
            hi_o[128 + 16 * j : 144 + 16 * j, :] = p1_o[
                ROWS - 16 : ROWS, 256 * j : 256 * (j + 1)
            ]


def gate_kernel(xs, rs, wg, gate_o):
    gate_o[...] = (dot(xs[...], wg[...]) * rs[:, 0:1]).astype(bf16)


def steps_kernel(st, bias, rate, offset, rows_o, col_o):
    unit = iota((16, 1), 0)

    def as_column(table):
        value = jnp.zeros((16, 1), f32)
        for d in range(2):
            for h in range(HEADS):
                value = jnp.where(unit == 8 * d + h, table[d, h], value)
        return value

    v = st[...] + as_column(bias)
    step = jnp.maximum(v, 0.0) + jnp.log1p(jnp.exp(-jnp.abs(v)))
    decay = -as_column(rate) * step + offset[...]
    count = 1024 // BLOCK
    parts = [decay[:, BLOCK * s : BLOCK * (s + 1)] for s in range(count)]
    stacked = jnp.concatenate(parts, axis=0)
    hi, mid, lo = split3(stacked)
    row = iota((128, 256), 0)
    column = iota((128, 256), 1)
    prefix = (column < 128) & (row <= column)
    suffix = (column >= 128) & (row >= column - 128)
    sums = jnp.where(prefix | suffix, 1.0, 0.0).astype(bf16)
    total = dot(hi.astype(bf16), sums) + dot(mid.astype(bf16), sums) + dot(lo.astype(bf16), sums)
    for s in range(count):
        c = jnp.concatenate(
            [total[16 * s : 16 * s + 8, 0:128], total[16 * s + 8 : 16 * s + 16, 128:256]], axis=0
        )
        steps = step[:, BLOCK * s : BLOCK * (s + 1)]
        last = jnp.concatenate([c[0:8, 127:128], c[8:16, 0:1]], axis=0)
        factor = steps * jnp.exp(last - c)
        raised = jnp.exp(c)
        rows_o[s, 0:16, :] = jnp.log(steps) - c
        rows_o[s, 16:24, :] = steps[0:8] + steps[8:16]
        factor_hi, factor_lo = split2(factor)
        raised_hi, raised_lo = split2(raised)
        packed = jnp.concatenate(
            [c, factor_hi, factor_lo, raised_hi, raised_lo, jnp.zeros((48, 128), f32)], axis=0
        )
        col_o[BLOCK * s : BLOCK * (s + 1), :] = packed.T


def mixer_kernel(
    p1, lo, hi, ti, tb, tc, rows, col, expand, pick,
    within_o, cmat_o, add_o, tot_o, pack_o,
    xpad, run_f, run_b, prod_f, prod_b, score, weight, bs, inner_s, loaded,
):
    i = pl.program_id(0)
    start = pl.multiple_of(i * SPAN, SPAN)
    final = pl.num_programs(0) - 1

    @pl.when(i == 0)
    def _():
        run_f[...] = jnp.zeros_like(run_f)
        run_b[...] = jnp.zeros_like(run_b)
        prod_f[...] = jnp.ones_like(prod_f)
        prod_b[...] = jnp.ones_like(prod_b)
        for j in range(4):
            xpad[0:8, 256 * j : 256 * (j + 1)] = lo[128 + 16 * j : 144 + 16 * j, :].astype(f32)[
                8:16
            ]

    @pl.when(i > 0)
    def _():
        before = pl.multiple_of(jnp.maximum(start - 16, 0), 16)
        xpad[0:8, :] = p1[pl.ds(before, 16), :].astype(f32)[8:16]

    @pl.when(i < final)
    def _():
        after = pl.multiple_of(jnp.minimum(start + SPAN, 1008), 16)
        xpad[SPAN + 8 : SPAN + 16, :] = p1[pl.ds(after, 16), :].astype(f32)[0:8]

    @pl.when(i == final)
    def _():
        for j in range(4):
            xpad[SPAN + 8 : SPAN + 16, 256 * j : 256 * (j + 1)] = hi[
                128 + 16 * j : 144 + 16 * j, :
            ].astype(f32)[0:8]

    xpad[8 : SPAN + 8, :] = p1[pl.ds(start, SPAN), :].astype(f32)

    def convolved(taps, low, high):
        table = taps[...].astype(f32)
        total = table[0:1] * xpad[6 : 6 + SPAN, low:high]
        for j in range(1, CONV):
            total = total + table[j : j + 1] * xpad[6 + j : 6 + j + SPAN, low:high]
        return (total / (1.0 + jnp.exp(-total))).astype(bf16)

    bs[...] = convolved(tb, 0 + 512, 768)
    cmat_o[...] = convolved(tc, 768, 1024)
    count = SPAN // BLOCK
    spans = [slice(BLOCK * k, BLOCK * (k + 1)) for k in range(count)]
    groups = [slice(128 * g, 128 * (g + 1)) for g in range(2)]
    for k in range(count):
        for g in range(2):
            score[k, g] = dot_rt(cmat_o[spans[k], groups[g]], bs[spans[k], groups[g]])
    inner_s[...] = convolved(ti, 0, 512)
    flipped = bs[...].astype(f32).T.astype(bf16)
    factors = col[...].astype(bf16)
    tot_f, tot_b = [], []
    for k in range(count):
        widened = dot(factors[spans[k], :], expand[...])
        inner_wide = inner_s[spans[k], :].astype(f32)
        loaded[spans[k], 0:512] = (inner_wide * widened[:, 0:512]).astype(bf16)
        loaded[spans[k], 512:1024] = (inner_wide * widened[:, 512:1024]).astype(bf16)
        tot_f.append(widened[127:128, 1024:1536])
        tot_b.append(widened[0:1, 1536:2048])
        tot_o[pl.ds(i * count + k, 1), 0:512] = tot_f[k]
        tot_o[pl.ds(i * count + k, 1), 512:1024] = tot_b[k]
    for k in range(count):
        for g in range(2):
            for d in range(2):
                cols = slice(256 * g, 256 * (g + 1))
                cols_d = slice(512 * d + 256 * g, 512 * d + 256 * (g + 1))
                add_o[k, d, :, cols] = dot(flipped[groups[g], spans[k]], loaded[spans[k], cols_d])
    row = iota((128, 128), 0)
    column = iota((128, 128), 1)
    causal = row >= column
    diagonal = row == column
    for k in range(count):
        for h in range(HEADS):
            forward = col[spans[k], h : h + 1] + rows[k, h : h + 1, :]
            backward = col[spans[k], 8 + h : 9 + h] + rows[k, 8 + h : 9 + h, :]
            spread = jnp.exp(jnp.where(causal, forward, backward))
            spread = jnp.where(diagonal, rows[k, 16 + h : 17 + h, :], spread)
            weight[k, h // 2, :, 128 * (h % 2) : 128 * (h % 2) + 128] = (
                score[k, h // 4] * spread
            ).astype(bf16)
    low_lane = iota((1, 128), 1) < HEAD
    for k in range(count):
        for pair in range(HEADS // 2):
            both = inner_s[spans[k], 128 * pair : 128 * (pair + 1)]
            zero = jnp.zeros_like(both)
            right = jnp.concatenate(
                [jnp.where(low_lane, both, zero), jnp.where(low_lane, zero, both)], axis=0
            )
            within_o[spans[k], 128 * pair : 128 * (pair + 1)] = dot(weight[k, pair], right)
    for k in range(count):
        for c in range(4):
            cols = slice(128 * c, 128 * (c + 1))
            run_f[:, cols] = tot_f[k][:, cols] * run_f[:, cols] + add_o[k, 0, :, cols]
            run_b[:, cols] = run_b[:, cols] + prod_b[:, cols] * add_o[k, 1, :, cols]
        prod_f[...] = prod_f[...] * tot_f[k]
        prod_b[...] = prod_b[...] * tot_b[k]

    @pl.when(i == final)
    def _():
        levels = jnp.concatenate([prod_f[...], prod_b[...]], axis=0)
        hi_l, mid_l, lo_l = split3(levels)
        joined = jnp.concatenate([hi_l, mid_l, lo_l], axis=1).astype(bf16)
        sent = dot(joined, pick[...])
        sent = jnp.concatenate(
            [jnp.broadcast_to(sent[0:1], (8, 128)), jnp.broadcast_to(sent[1:2], (8, 128))], axis=0
        ).astype(bf16)
        for j in range(16):
            pack_o[j, :, 0:512] = jnp.concatenate(
                [run_f[8 * j : 8 * j + 8, :], run_b[8 * j : 8 * j + 8, :]], axis=0
            ).astype(bf16)
            pack_o[j, :, 512:640] = sent


def carry_kernel(arrived, start, spread, out, wide, held):
    sp = lax.axis_index("sp")
    for j in range(16):
        wide[j] = dot(arrived[j, :, 512:640], spread[...])
    state = start[0, pl.ds(sp, 1)][0]
    for j in range(16):
        held[j, 0:8, :] = state
        state = wide[j, 0:8, :] * state + arrived[j, :, 0:512].astype(f32)[0:8]
    state = start[1, pl.ds(sp, 1)][0]
    for j in reversed(range(16)):
        held[j, 8:16, :] = state
        state = wide[j, 8:16, :] * state + arrived[j, :, 0:512].astype(f32)[8:16]
    for j in range(16):
        out[j] = held[j].astype(bf16)


def attend_kernel(q, kv, lo, hi, sink, out, keys, vals, score, weight):
    i = pl.program_id(0)
    sp = lax.axis_index("sp")
    low_lane = iota((1, 128), 1) < HEAD

    def place(first, count, pairs):
        kk = pairs[:, 0:128].astype(f32)
        kr = pltpu.roll(kk, 64, 1)
        span = slice(first, first + count)
        keys[0, span, :] = jnp.where(low_lane, kk, kr).astype(bf16)
        keys[1, span, :] = jnp.where(low_lane, kr, kk).astype(bf16)
        flipped = pairs[:, 128:256].astype(f32).T.astype(bf16)
        ones = jnp.ones((HEAD, count), bf16)
        for g in range(2):
            vals[g, 0:HEAD, span] = flipped[HEAD * g : HEAD * (g + 1)]
            vals[g, HEAD:128, span] = ones

    @pl.when(i == 0)
    def _():
        place(0, 128, lo[0:128, :])
        place(128, 1024, kv[...])
        place(1152, 128, hi[0:128, :])

    count = SPAN // BLOCK
    starts = [pl.multiple_of(i * SPAN + BLOCK * k, BLOCK) for k in range(count)]
    items = [(k, g, j) for k in range(count) for g in range(2) for j in range(2)]
    for n, (k, g, j) in enumerate(items):
        base = 256 * g + 128 * j
        tile = q[BLOCK * k : BLOCK * (k + 1), base : base + 128].astype(f32) * 0.125
        tile = tile.astype(bf16)
        zero = jnp.zeros_like(tile)
        both = jnp.concatenate(
            [jnp.where(low_lane, tile, zero), jnp.where(low_lane, zero, tile)], axis=0
        )
        score[n] = dot_rt(keys[g, pl.ds(starts[k], 384), :], both)
    key = iota((128, 128), 0)
    query = iota((128, 128), 1)
    biases = []
    for k in range(count):
        b = i * count + k
        no_left = (b == 0) & (sp == 0)
        no_right = (b == 7) & (sp == lax.axis_size("sp") - 1)
        left_from = jnp.where(no_left, 128, 0)
        right_to = jnp.where(no_right, -1, 127)
        left = jnp.where((key >= query) & (key >= left_from), 0.0, -1e30)
        right = jnp.where((key <= query) & (key <= right_to), 0.0, -1e30)
        biases.append((left, right))
    sinks = []
    for n, (k, g, j) in enumerate(items):
        left, right = biases[k]
        for half in range(2):
            lanes = slice(128 * half, 128 * (half + 1))
            sink_h = jnp.full((1, 128), sink[4 * g + 2 * j + half], f32)
            low = score[n, 0:128, lanes] + left
            middle = score[n, 128:256, lanes]
            high = score[n, 256:384, lanes] + right
            highest = jnp.max(jnp.maximum(jnp.maximum(low, middle), high), axis=0, keepdims=True)
            highest = jnp.maximum(highest, sink_h)
            weight[n, 0:128, lanes] = jnp.exp(low - highest).astype(bf16)
            weight[n, 128:256, lanes] = jnp.exp(middle - highest).astype(bf16)
            weight[n, 256:384, lanes] = jnp.exp(high - highest).astype(bf16)
            sinks.append(jnp.exp(sink_h - highest))
    results = [
        dot(vals[g, :, pl.ds(starts[k], 384)], weight[n]) for n, (k, g, j) in enumerate(items)
    ]
    for n, (k, g, j) in enumerate(items):
        finals = []
        for half in range(2):
            lanes = slice(128 * half, 128 * (half + 1))
            denominator = results[n][HEAD : HEAD + 1, lanes] + sinks[2 * n + half]
            finals.append(results[n][0:HEAD, lanes] * (1.0 / denominator))
        base = 256 * g + 128 * j
        out[BLOCK * k : BLOCK * (k + 1), base : base + 128] = (
            jnp.concatenate(finals, axis=0).T.astype(bf16)
        )


def finish_kernel(arrived, add, tot, within, cmat, gate, col, expand, gain, out, entering, made):
    i = pl.program_id(0)

    @pl.when(i == 0)
    def _():
        for c in range(4):
            cols = slice(128 * c, 128 * (c + 1))
            cols_b = slice(512 + 128 * c, 512 + 128 * (c + 1))
            both = [arrived[j, :, cols].astype(f32) for j in range(16)]
            state = jnp.concatenate([slab[0:8] for slab in both], axis=0)
            for b in range(8):
                entering[b, :, cols] = state.astype(bf16)
                if b < 7:
                    state = tot[b : b + 1, cols] * state + add[b, 0, :, cols]
            state = jnp.concatenate([slab[8:16] for slab in both], axis=0)
            for b in reversed(range(8)):
                entering[b, :, cols_b] = state.astype(bf16)
                if b > 0:
                    state = tot[b : b + 1, cols_b] * state + add[b, 1, :, cols]

    count = SPAN // BLOCK
    for k in range(count):
        span = slice(BLOCK * k, BLOCK * (k + 1))
        for g in range(2):
            for d in range(2):
                cols = slice(512 * d + 256 * g, 512 * d + 256 * (g + 1))
                made[span, cols] = dot(
                    cmat[span, 128 * g : 128 * (g + 1)], entering[i * count + k, :, cols]
                )
    for k in range(count):
        span = slice(BLOCK * k, BLOCK * (k + 1))
        widened = dot(col[span, :].astype(bf16), expand[:, 1024:2048])
        for g in range(2):
            cols = slice(256 * g, 256 * (g + 1))
            cols_b = slice(512 + 256 * g, 512 + 256 * (g + 1))
            total = within[span, cols] + widened[:, cols] * made[span, cols]
            total = total + widened[:, cols_b] * made[span, cols_b]
            gates = gate[span, cols].astype(f32)
            gated = total * (gates / (1.0 + jnp.exp(-gates)))
            mean = jnp.mean(gated * gated, axis=1, keepdims=True)
            out[span, cols] = (gated * lax.rsqrt(mean + EPS) * gain[:, cols]).astype(bf16)


def output_kernel(attn, mixed, wa, ws, out, *, swapped):
    t = lax.axis_index("tp")
    half = 1 - t if swapped else t
    rows = pl.ds(pl.multiple_of(half * ROWS, ROWS), ROWS)
    out[...] = (dot(attn[rows, :], wa[...]) + dot(mixed[rows, :], ws[...])).astype(bf16)


def call(kernel, name, grid, in_specs, out_specs, out_shape, scratch=(), flops=0, nbytes=0, mib=40):
    return pl.pallas_call(
        kernel,
        name=name,
        grid_spec=pltpu.PrefetchScalarGridSpec(
            num_scalar_prefetch=0,
            grid=grid,
            in_specs=in_specs,
            out_specs=out_specs,
            scratch_shapes=list(scratch),
        ),
        out_shape=out_shape,
        cost_estimate=pl.CostEstimate(flops=flops, transcendentals=0, bytes_accessed=nbytes),
        compiler_params=pltpu.CompilerParams(
            dimension_semantics=("arbitrary",) * len(grid), vmem_limit_bytes=mib << 20
        ),
    )


def local(
    inputs, mix_gain, w_query, w_key, w_value, query_gain, key_gain, sink_logit, w_inner, w_bmat,
    w_cmat, w_gate, w_step, conv_inner, conv_bmat, conv_cmat, step_bias, decay_rate, decay_offset,
    start_state, group_gain, w_out_attn, w_out_state,
):
    sp_count = lax.axis_size("sp")
    swap = [(0, 1), (1, 0)]
    other = lax.ppermute(inputs, "tp", swap)

    cosb, sinb = rotation_tables(np.arange(128) * BLOCK)
    cosi, sini = rotation_tables(np.arange(BLOCK))
    scalar = pl.BlockSpec(memory_space=pltpu.SMEM)
    rows2 = lambda width: pl.BlockSpec((ROWS, width), lambda i: (i, 0))
    grid = (1024 // ROWS,)
    q_rot, kv, p1, step_t, xs, rs, lo_edge, hi_edge = call(
        project_kernel, "project", grid,
        [
            rows2(HALF), VM, once((1, D)), once((D, 512)), once((D, 128)), once((D, 128)),
            once((D, 512)), once((D, 256)), once((D, 256)), once((16, D)), once((1, 64)),
            once((1, 64)), once((128, 128)), once((128, 128)), once((128, 128)), once((128, 128)),
        ],
        [
            rows2(512), rows2(256), rows2(1024), pl.BlockSpec((16, ROWS), lambda i: (0, i)),
            rows2(D), rows2(128), whole((192, 256)), whole((192, 256)),
        ],
        [
            hbm((1024, 512), bf16), hbm((1024, 256), bf16), hbm((1024, 1024), bf16),
            hbm((16, 1024), f32), hbm((1024, D), bf16), hbm((1024, 128), f32),
            sds((192, 256), bf16), sds((192, 256), bf16),
        ],
        scratch=[
            pltpu.VMEM((D, 256), bf16), pltpu.VMEM((5, ROWS, 128), f32),
            pltpu.VMEM((2, 5, ROWS, 128), bf16),
        ],
        flops=2 * 1024 * D * 1808, nbytes=20 << 20, mib=48,
    )(
        far(inputs), near(other), far(mix_gain.reshape(1, D)), far(w_query), far(w_key),
        far(w_value), far(w_inner), far(w_bmat), far(w_cmat),
        far(w_step.transpose(1, 2, 0).reshape(16, D)), far(query_gain.reshape(1, HEAD)),
        far(key_gain.reshape(1, HEAD)), far(cosb), far(sinb), far(cosi), far(sini),
    )

    forward = [(i, i + 1) for i in range(sp_count - 1)]
    backward = [(i + 1, i) for i in range(sp_count - 1)]
    lo = lax.ppermute(hi_edge, "sp", forward)
    hi = lax.ppermute(lo_edge, "sp", backward)

    rows, col = call(
        steps_kernel, "steps", (1,),
        [whole((16, 1024)), scalar, scalar, whole((16, 1024))],
        [whole((8, 24, 128)), whole((1024, 128))],
        [hbm((8, 24, 128), f32), hbm((1024, 128), f32)], flops=1 << 24, nbytes=1 << 20,
    )(far(step_t), step_bias, decay_rate, far(decay_offset.reshape(1024, 16).T))

    lane = np.arange(1024)
    unit = lane // HEAD
    expand = np.zeros((128, 2048), np.float32)
    for u in range(16):
        for base, shift in ((16, 0), (32, 0), (48, 1024), (64, 1024)):
            expand[base + u, shift : shift + 1024] = unit == u
    expand = jnp.asarray(expand, bf16)
    pick = np.zeros((1536, 128), np.float32)
    for part in range(3):
        for h in range(HEADS):
            pick[512 * part + HEAD * h, 8 * part + h] = 1
    pick = jnp.asarray(pick, bf16)
    spread = np.zeros((128, 512), np.float32)
    for j in range(24):
        spread[j] = (lane[:512] // HEAD) == (j % 8)
    spread = jnp.asarray(spread, bf16)

    count = SPAN // BLOCK
    blocks = (1024 // SPAN,)
    rows1 = lambda width: pl.BlockSpec((SPAN, width), lambda b: (b, 0))
    within, cmat, add, tot, pack = call(
        mixer_kernel, "mixer", blocks,
        [
            once((1024, 1024)), VM, VM, once((CONV, 512)), once((CONV, 256)), once((CONV, 256)),
            pl.BlockSpec((count, 24, 128), lambda b: (b, 0, 0)), rows1(128), once((128, 2048)),
            once((1536, 128)),
        ],
        [
            rows1(512), rows1(256), pl.BlockSpec((count, 2, 128, 512), lambda b: (b, 0, 0, 0)),
            whole((8, 1024)), whole((16, 16, 640)),
        ],
        [
            hbm((1024, 512), f32), hbm((1024, 256), bf16), hbm((8, 2, 128, 512), f32),
            hbm((8, 1024), f32), sds((16, 16, 640), bf16),
        ],
        scratch=[
            pltpu.VMEM((SPAN + 16, 1024), f32), pltpu.VMEM((128, 512), f32),
            pltpu.VMEM((128, 512), f32), pltpu.VMEM((1, 512), f32), pltpu.VMEM((1, 512), f32),
            pltpu.VMEM((count, 2, 128, 128), f32), pltpu.VMEM((count, 4, 128, 256), bf16),
            pltpu.VMEM((SPAN, 256), bf16), pltpu.VMEM((SPAN, 512), bf16),
            pltpu.VMEM((SPAN, 1024), bf16),
        ],
        flops=1 << 30, nbytes=12 << 20,
    )(
        far(p1), near(lo), near(hi), conv_inner, conv_bmat, conv_cmat, far(rows), far(col),
        far(expand), far(pick),
    )

    arrived = lax.all_to_all(pack, "sp", 0, 0, tiled=True)
    attention = call(
        attend_kernel, "attend", blocks,
        [rows1(512), once((1024, 256)), VM, VM, scalar], rows1(512), hbm((1024, 512), bf16),
        scratch=[
            pltpu.VMEM((2, 1280, 128), bf16), pltpu.VMEM((2, 128, 1280), bf16),
            pltpu.VMEM((4 * count, 384, 256), f32), pltpu.VMEM((4 * count, 384, 256), bf16),
        ],
        flops=1 << 31, nbytes=4 << 20,
    )(far(q_rot), far(kv), near(lo), near(hi), sink_logit)
    start_t = start_state.reshape(2, 512, 16, 8).transpose(0, 2, 3, 1)
    arrived, attention, start_t = lax.optimization_barrier((arrived, attention, start_t))
    carried = call(
        carry_kernel, "carry", (1,), [VM, whole((2, 16, 8, 512)), whole((128, 512))],
        whole((16, 16, 512)), sds((16, 16, 512), bf16),
        scratch=[pltpu.VMEM((16, 16, 512), f32), pltpu.VMEM((16, 16, 512), f32)],
        flops=1 << 22, nbytes=1 << 20,
    )(near(arrived), start_t, far(spread))
    carried, xs = lax.optimization_barrier((carried, xs))
    returned = lax.all_to_all(carried, "sp", 0, 0, tiled=True)
    gate = call(
        gate_kernel, "gate", grid, [rows2(D), rows2(128), once((D, 512))], rows2(512),
        hbm((1024, 512), bf16), flops=2 * 1024 * D * 512, nbytes=8 << 20,
    )(far(xs), far(rs), far(w_gate))
    returned, gate = lax.optimization_barrier((returned, gate))
    state_out = call(
        finish_kernel, "finish", blocks,
        [
            VM, once((8, 2, 128, 512)), once((8, 1024)), rows1(512), rows1(256), rows1(512),
            rows1(128), once((128, 2048)), once((1, 512)),
        ],
        rows1(512), sds((1024, 512), bf16),
        scratch=[pltpu.VMEM((8, 128, 1024), bf16), pltpu.VMEM((SPAN, 1024), f32)],
        flops=1 << 29, nbytes=10 << 20, mib=24,
    )(
        near(returned), far(add), far(tot), far(within), far(cmat), far(gate), far(col),
        far(expand), group_gain.reshape(1, 512),
    )

    def projected(swapped):
        weight = pl.BlockSpec((512, 512), lambda n: (0, n))
        return call(
            functools.partial(output_kernel, swapped=swapped), "output", (4,),
            [once((1024, 512)), once((1024, 512)), weight, weight],
            pl.BlockSpec((ROWS, 512), lambda n: (0, n)), sds((ROWS, D), bf16),
            flops=2 * 512 * 1024 * D, nbytes=8 << 20, mib=16,
        )(attention, state_out, w_out_attn, w_out_state)

    sent = projected(True)
    received = lax.ppermute(sent, "tp", swap)
    kept = projected(False)
    return (kept.astype(f32) + received.astype(f32)).astype(bf16)


def solution(mesh):
    return jax.shard_map(
        local,
        mesh=mesh,
        in_specs=(
            P(("fs", "sp"), "tp"), P(), P(None, "tp"), P(None, "tp"), P(None, "tp"), P(), P(),
            P("tp"), P(None, "tp"), P(None, "tp"), P(None, "tp"), P(None, "tp"),
            P(None, None, "tp"), P(None, "tp"), P(None, "tp"), P(None, "tp"), P(None, "tp"),
            P(None, "tp"), P("sp", None, "tp"), P("fs", "tp", None, None), P("tp"),
            P("tp", None), P("tp", None),
        ),
        out_specs=P(("fs", "sp", "tp"), None),
        check_vma=False,
    )
```

```python
import functools

import jax
import jax.numpy as jnp
import numpy as np
from jax import lax
from jax.experimental import pallas as pl
from jax.experimental.pallas import tpu as pltpu
from jax.sharding import PartitionSpec as P

D = 2048
HALF = 1024
HEAD = 64
STATE = 128
CONV = 5
BLOCK = 128
EPS = 1e-06
BASE = 10000.0
HEADS = 8
LOG2E = 1.4426950408889634
ROWS = 512
PART = 256
SPAN = 256
f32 = jnp.float32
bf16 = jnp.bfloat16


def dot(a, b):
    return jnp.dot(a, b, preferred_element_type=f32)


def dot_rt(a, b):
    return lax.dot_general(a, b, (((1,), (1,)), ((), ())), preferred_element_type=f32)


def split2(v):
    hi = v.astype(bf16).astype(f32)
    return hi, (v - hi).astype(bf16).astype(f32)


def split3(v):
    hi = v.astype(bf16).astype(f32)
    rest = v - hi
    mid = rest.astype(bf16).astype(f32)
    return hi, mid, (rest - mid).astype(bf16).astype(f32)


def iota(shape, dim):
    return lax.broadcasted_iota(jnp.int32, shape, dim)


def whole(shape):
    zeros = (0,) * len(shape)
    return pl.BlockSpec(shape, lambda *_: zeros)


def once(shape):
    zeros = (0,) * len(shape)
    return pl.BlockSpec(shape, lambda *_: zeros, pipeline_mode=pl.Buffered(1))


def near(value):
    return pltpu.with_memory_space_constraint(value, pltpu.VMEM)


def far(value):
    return pltpu.with_memory_space_constraint(value, pltpu.HBM)


VM = pl.BlockSpec(memory_space=pltpu.VMEM)


def hbm(shape, dtype):
    return pltpu.HBM(shape, dtype)


def vmem(shape, dtype):
    return pltpu.VMEM(shape, dtype)


def sds(shape, dtype):
    return jax.ShapeDtypeStruct(shape, dtype)


def rotation_tables(positions):
    lane = np.arange(128) % 32
    freq = BASE ** (-lane.astype(np.float64) / 32)
    angles = positions.astype(np.float64)[:, None] * freq[None, :]
    return np.cos(angles).astype(np.float32), np.sin(angles).astype(np.float32)


def early_kernel(
    xo, gain, wq, wk, wv, wi, wb, wc, wg, ws,
    ss_o, aq, akv, ai, ab, ac, ag, at, pq, pkv, pi, pb, pc, pg,
    oq, okv, oi, ob, oc, og, xs_o, sems,
):
    i = pl.program_id(0)
    t = lax.axis_index("tp")
    own = pl.multiple_of(t * HALF, HALF)
    peer = pl.multiple_of((1 - t) * HALF, HALF)

    def copies(first, targets, base):
        q, kv, inner, bm, cm, gm = targets
        pairs = (
            (wq, q), (wk, kv.at[:, 0:128]), (wv, kv.at[:, 128:256]), (wi, inner), (wb, bm),
            (wc, cm), (wg, gm),
        )
        return [
            pltpu.make_async_copy(w.at[pl.ds(first, HALF), :], target, sems.at[base + n])
            for n, (w, target) in enumerate(pairs)
        ]

    mine = copies(own, (oq, okv, oi, ob, oc, og), 0)
    others = copies(peer, (pq, pkv, pi, pb, pc, pg), 7)

    @pl.when(i == 0)
    def _():
        for copy in mine:
            copy.start()
        for copy in others:
            copy.start()

    own_x = xo[...].astype(f32)
    rows = pl.ds(pl.multiple_of(i * PART, PART), PART)
    xs_o[...] = (own_x * gain[:, pl.ds(own, HALF)]).astype(bf16)
    ss_o[rows, :] = jnp.broadcast_to(jnp.sum(own_x * own_x, axis=1, keepdims=True), (PART, 128))

    @pl.when(i == 0)
    def _():
        for copy in mine:
            copy.wait()

    for w, acc in ((oq, aq), (okv, akv), (oi, ai), (ob, ab), (oc, ac), (og, ag)):
        acc[rows, :] = dot(xs_o[...], w[...])
    at[rows, :] = dot_rt(xs_o[...], ws[:, pl.ds(own, HALF)])

    @pl.when(i == pl.num_programs(0) - 1)
    def _():
        for copy in others:
            copy.wait()


def swapped(value):
    first = (iota((1, 128), 1) % HEAD) < (HEAD // 2)
    return jnp.where(first, pltpu.roll(value, 96, 1), pltpu.roll(value, 32, 1))


def norm_and_rotate(tiles, outs, gain, first_block, tables, means, scaled):
    cosb, sinb, cosi, sini = tables
    same = (iota((128, 128), 0) // HEAD) == (iota((128, 128), 1) // HEAD)
    averaging = jnp.where(same, 1.0 / HEAD, 0.0).astype(bf16)
    for j, tile in enumerate(tiles):
        values = tile[...].astype(f32)
        scaled[j] = (values * values).astype(bf16)
    for j in range(len(tiles)):
        means[j] = dot(scaled[j], averaging)
    first = (iota((1, 128), 1) % HEAD) < (HEAD // 2)
    wide = jnp.broadcast_to(jnp.concatenate([gain, gain], axis=1), (8, 128))
    gain_a, gain_b = wide[0:1], swapped(wide)[0:1]
    for s in range(tiles[0].shape[0] // BLOCK):
        span = slice(BLOCK * s, BLOCK * (s + 1))
        cb = cosb[pl.ds(first_block + s, 1), :]
        sb = sinb[pl.ds(first_block + s, 1), :]
        cosine = (cb * cosi[...] - sb * sini[...]) * gain_a
        sine = (sb * cosi[...] + cb * sini[...]) * gain_b
        sine = jnp.where(first, -sine, sine)
        for j, tile in enumerate(tiles):
            y = tile[span, :].astype(f32)
            y = (y * cosine + swapped(y) * sine) * lax.rsqrt(means[j, span, :] + EPS)
            outs[j][span, :] = y.astype(bf16)


def project_kernel(
    xp, gain, ws, kg, cosb, sinb, cosi, sini,
    ss, aq, akv, ai, ab, ac, ag, at, wq, wkv, wi, wb, wc, wg,
    q_o, kv_o, p1_o, pc_o, st_o, gate_o, lo_o, hi_o, means, scaled, xs_o,
):
    i = pl.program_id(0)
    t = lax.axis_index("tp")
    sp = lax.axis_index("sp")
    peer = pl.multiple_of((1 - t) * HALF, HALF)
    rows = pl.ds(pl.multiple_of(i * ROWS, ROWS), ROWS)
    peer_x = xp[rows, :].astype(f32)
    xs_o[...] = (peer_x * gain[:, pl.ds(peer, HALF)]).astype(bf16)
    squares = ss[rows, 0:1] + jnp.sum(peer_x * peer_x, axis=1, keepdims=True)
    rs = lax.rsqrt(squares * (1.0 / D) + EPS)

    def proj(w, acc):
        return (dot(xs_o[...], w[...]) + acc[rows, :]) * rs

    kv_o[...] = proj(wkv, akv).astype(bf16)
    p1_o[rows, 0:512] = proj(wi, ai).astype(bf16)
    tile = [kv_o.at[:, 0:128]]
    block = sp * 8 + i * (ROWS // BLOCK)
    norm_and_rotate(tile, tile, kg[...], block, (cosb, sinb, cosi, sini), means, scaled)
    p1_o[rows, 512:768] = proj(wb, ab).astype(bf16)
    pc_o[...] = proj(wc, ac).astype(bf16)
    q_o[rows, :] = proj(wq, aq).astype(bf16)
    gate_o[...] = proj(wg, ag).astype(bf16)
    steps = (dot_rt(xs_o[...], ws[:, pl.ds(peer, HALF)]) + at[rows, :]) * rs
    st_o[...] = jnp.concatenate([steps, jnp.zeros((ROWS, 112), f32)], axis=1).T[0:16, :]

    @pl.when(i == 0)
    def _():
        lo_o[0:128, :] = kv_o[0:128, :]
        for j in range(3):
            lo_o[128 + 16 * j : 144 + 16 * j, :] = p1_o[0:16, 256 * j : 256 * (j + 1)]
        lo_o[176:192, :] = pc_o[0:16, :]

    @pl.when(i == pl.num_programs(0) - 1)
    def _():
        hi_o[0:128, :] = kv_o[ROWS - 128 : ROWS, :]
        for j in range(3):
            hi_o[128 + 16 * j : 144 + 16 * j, :] = p1_o[
                1024 - 16 : 1024, 256 * j : 256 * (j + 1)
            ]
        hi_o[176:192, :] = pc_o[ROWS - 16 : ROWS, :]


def steps_kernel(
    st, bias, rate, offset, q, qg, cosb, sinb, cosi, sini, rows_o, col_o, q_o, means, scaled
):
    tiles = [q.at[:, 128 * j : 128 * (j + 1)] for j in range(4)]
    outs = [q_o.at[:, 128 * j : 128 * (j + 1)] for j in range(4)]
    gain = qg[...] * (HEAD**-0.5 * LOG2E)
    first_block = lax.axis_index("sp") * 8
    norm_and_rotate(tiles, outs, gain, first_block, (cosb, sinb, cosi, sini), means, scaled)
    unit = iota((16, 1), 0)

    def as_column(table):
        value = jnp.zeros((16, 1), f32)
        for d in range(2):
            for h in range(HEADS):
                value = jnp.where(unit == 8 * d + h, table[d, h], value)
        return value

    v = st[...] + as_column(bias)
    step = jnp.maximum(v, 0.0) + jnp.log1p(jnp.exp(-jnp.abs(v)))
    decay = -as_column(rate) * step + offset[...]
    count = 1024 // BLOCK
    parts = [decay[:, BLOCK * s : BLOCK * (s + 1)] for s in range(count)]
    stacked = jnp.concatenate(parts, axis=0)
    hi, mid, lo = split3(stacked)
    row = iota((128, 256), 0)
    column = iota((128, 256), 1)
    prefix = (column < 128) & (row <= column)
    suffix = (column >= 128) & (row >= column - 128)
    sums = jnp.where(prefix | suffix, 1.0, 0.0).astype(bf16)
    total = dot(hi.astype(bf16), sums) + dot(mid.astype(bf16), sums) + dot(lo.astype(bf16), sums)
    for s in range(count):
        c = jnp.concatenate(
            [total[16 * s : 16 * s + 8, 0:128], total[16 * s + 8 : 16 * s + 16, 128:256]], axis=0
        )
        steps = step[:, BLOCK * s : BLOCK * (s + 1)]
        last = jnp.concatenate([c[0:8, 127:128], c[8:16, 0:1]], axis=0)
        factor = steps * jnp.exp(last - c)
        raised = jnp.exp(c)
        rows_o[s, 0:16, :] = (jnp.log(steps) - c) * LOG2E
        rows_o[s, 16:24, :] = steps[0:8] + steps[8:16]
        factor_hi, factor_lo = split2(factor)
        raised_hi, raised_lo = split2(raised)
        packed = jnp.concatenate(
            [c * LOG2E, factor_hi, factor_lo, raised_hi, raised_lo, jnp.zeros((48, 128), f32)],
            axis=0,
        )
        col_o[BLOCK * s : BLOCK * (s + 1), :] = packed.T


def frame(p1, lo, hi, xpad, first_piece):
    i = pl.program_id(0)
    start = pl.multiple_of(i * SPAN, SPAN)
    final = pl.num_programs(0) - 1
    chunks = xpad.shape[0]
    after_rows = slice(SPAN + 8, SPAN + 16)

    @pl.when(i == 0)
    def _():
        for c in range(chunks):
            top = 128 + 16 * (first_piece + c // 2)
            lanes = slice(128 * (c % 2), 128 * (c % 2) + 128)
            xpad[c, 0:8, :] = lo[top : top + 16, lanes].astype(f32)[8:16]

    @pl.when(i > 0)
    def _():
        before = pl.multiple_of(jnp.maximum(start - 16, 0), 16)
        rim = p1[pl.ds(before, 16), :].astype(f32)[8:16]
        for c in range(chunks):
            xpad[c, 0:8, :] = rim[:, 128 * c : 128 * (c + 1)]

    @pl.when(i < final)
    def _():
        after = pl.multiple_of(jnp.minimum(start + SPAN, 1008), 16)
        rim = p1[pl.ds(after, 16), :].astype(f32)[0:8]
        for c in range(chunks):
            xpad[c, after_rows, :] = rim[:, 128 * c : 128 * (c + 1)]

    @pl.when(i == final)
    def _():
        for c in range(chunks):
            top = 128 + 16 * (first_piece + c // 2)
            lanes = slice(128 * (c % 2), 128 * (c % 2) + 128)
            xpad[c, after_rows, :] = hi[top : top + 16, lanes].astype(f32)[0:8]

    for c in range(chunks):
        xpad[c, 8 : SPAN + 8, :] = p1[pl.ds(start, SPAN), 128 * c : 128 * (c + 1)].astype(f32)


def convolve(xpad, taps, chunk, out):
    table = taps[...].astype(f32)
    for c in range(taps.shape[1] // 128):
        lanes = slice(128 * c, 128 * (c + 1))
        total = table[0:1, lanes] * xpad[chunk + c, 6 : 6 + SPAN, :]
        for j in range(1, CONV):
            total = total + table[j : j + 1, lanes] * xpad[chunk + c, 6 + j : 6 + j + SPAN, :]
        out[:, lanes] = (total / (1.0 + jnp.exp(-total))).astype(bf16)


def mixer_kernel(
    p1, lo, hi, ti, tb, col, expand, pick,
    inner_s, bs, add_o, tot_o, pack_o,
    xpad, run_f, run_b, prod_f, prod_b, loaded, added,
):
    i = pl.program_id(0)

    @pl.when(i == 0)
    def _():
        run_f[...] = jnp.zeros_like(run_f)
        run_b[...] = jnp.zeros_like(run_b)
        prod_f[...] = jnp.ones_like(prod_f)
        prod_b[...] = jnp.ones_like(prod_b)

    frame(p1, lo, hi, xpad, 0)
    count = SPAN // BLOCK
    spans = [slice(BLOCK * k, BLOCK * (k + 1)) for k in range(count)]
    groups = [slice(128 * g, 128 * (g + 1)) for g in range(2)]
    convolve(xpad, tb, 4, bs)
    flipped = bs[...].astype(f32).T.astype(bf16)
    convolve(xpad, ti, 0, inner_s)
    factors = col[...].astype(bf16)
    tot_f, tot_b = [], []
    for k in range(count):
        widened = dot(factors[spans[k], :], expand[:, 0:1024])
        end = dot(factors[BLOCK * k + 112 : BLOCK * k + 128, :], expand[:, 1024:1536])
        begin = dot(factors[BLOCK * k : BLOCK * k + 16, :], expand[:, 1536:2048])
        inner_wide = inner_s[spans[k], :].astype(f32)
        loaded[spans[k], 0:512] = (inner_wide * widened[:, 0:512]).astype(bf16)
        loaded[spans[k], 512:1024] = (inner_wide * widened[:, 512:1024]).astype(bf16)
        tot_f.append(end[15:16])
        tot_b.append(begin[0:1])
        tot_o[pl.ds(i * count + k, 1), 0:512] = tot_f[k]
        tot_o[pl.ds(i * count + k, 1), 512:1024] = tot_b[k]
    for k in range(count):
        for g in range(2):
            for d in range(2):
                cols = slice(256 * g, 256 * (g + 1))
                cols_d = slice(512 * d + 256 * g, 512 * d + 256 * (g + 1))
                added[k, d, :, cols] = dot(flipped[groups[g], spans[k]], loaded[spans[k], cols_d])
    for k in range(count):
        for c in range(4):
            cols = slice(128 * c, 128 * (c + 1))
            run_f[:, cols] = tot_f[k][:, cols] * run_f[:, cols] + added[k, 0, :, cols]
            run_b[:, cols] = run_b[:, cols] + prod_b[:, cols] * added[k, 1, :, cols]
        add_o[k] = added[k].astype(bf16)
        prod_f[...] = prod_f[...] * tot_f[k]
        prod_b[...] = prod_b[...] * tot_b[k]

    @pl.when(i == pl.num_programs(0) - 1)
    def _():
        levels = jnp.concatenate([prod_f[...], prod_b[...]], axis=0)
        hi_l, mid_l, lo_l = split3(levels)
        joined = jnp.concatenate([hi_l, mid_l, lo_l], axis=1).astype(bf16)
        sent = dot(joined, pick[...])
        sent = jnp.concatenate(
            [jnp.broadcast_to(sent[0:1], (8, 128)), jnp.broadcast_to(sent[1:2], (8, 128))], axis=0
        ).astype(bf16)
        for j in range(16):
            pack_o[j, :, 0:512] = jnp.concatenate(
                [run_f[8 * j : 8 * j + 8, :], run_b[8 * j : 8 * j + 8, :]], axis=0
            ).astype(bf16)
            pack_o[j, :, 512:640] = sent


def within_kernel(
    pc, lo, hi, tc, rows, col, inner, bmat, within_o, cmat_o, xpad, score, weight
):
    frame(pc, lo, hi, xpad, 3)
    convolve(xpad, tc, 0, cmat_o)
    count = SPAN // BLOCK
    spans = [slice(BLOCK * k, BLOCK * (k + 1)) for k in range(count)]
    groups = [slice(128 * g, 128 * (g + 1)) for g in range(2)]
    for k in range(count):
        for g in range(2):
            score[k, g] = dot_rt(cmat_o[spans[k], groups[g]], bmat[spans[k], groups[g]])
    row = iota((128, 128), 0)
    column = iota((128, 128), 1)
    causal = row >= column
    diagonal = row == column
    for k in range(count):
        for h in range(HEADS):
            forward = col[spans[k], h : h + 1] + rows[k, h : h + 1, :]
            backward = col[spans[k], 8 + h : 9 + h] + rows[k, 8 + h : 9 + h, :]
            spread = jnp.exp2(jnp.where(causal, forward, backward))
            spread = jnp.where(diagonal, rows[k, 16 + h : 17 + h, :], spread)
            weight[k, h // 2, :, 128 * (h % 2) : 128 * (h % 2) + 128] = (
                score[k, h // 4] * spread
            ).astype(bf16)
    low_lane = iota((1, 128), 1) < HEAD
    for k in range(count):
        for pair in range(HEADS // 2):
            both = inner[spans[k], 128 * pair : 128 * (pair + 1)]
            zero = jnp.zeros_like(both)
            right = jnp.concatenate(
                [jnp.where(low_lane, both, zero), jnp.where(low_lane, zero, both)], axis=0
            )
            within_o[spans[k], 128 * pair : 128 * (pair + 1)] = dot(weight[k, pair], right)


def carry_kernel(arrived, start, spread, out, wide, held):
    sp = lax.axis_index("sp")
    for j in range(16):
        wide[j] = dot(arrived[j, :, 512:640], spread[...])
    state = start[0, pl.ds(sp, 1)][0]
    for j in range(16):
        held[j, 0:8, :] = state
        state = wide[j, 0:8, :] * state + arrived[j, :, 0:512].astype(f32)[0:8]
    state = start[1, pl.ds(sp, 1)][0]
    for j in reversed(range(16)):
        held[j, 8:16, :] = state
        state = wide[j, 8:16, :] * state + arrived[j, :, 0:512].astype(f32)[8:16]
    for j in range(16):
        out[j] = held[j].astype(bf16)


def attend_kernel(q, kv, lo, hi, sink, out, keys, vals, score, weight):
    i = pl.program_id(0)
    sp = lax.axis_index("sp")
    low_lane = iota((1, 128), 1) < HEAD

    def place(first, count, pairs):
        kk = pairs[:, 0:128].astype(f32)
        kr = pltpu.roll(kk, 64, 1)
        span = slice(first, first + count)
        keys[0, span, :] = jnp.where(low_lane, kk, kr).astype(bf16)
        keys[1, span, :] = jnp.where(low_lane, kr, kk).astype(bf16)
        flipped = pairs[:, 128:256].astype(f32).T.astype(bf16)
        ones = jnp.ones((HEAD, count), bf16)
        for g in range(2):
            vals[g, 0:HEAD, span] = flipped[HEAD * g : HEAD * (g + 1)]
            vals[g, HEAD:128, span] = ones

    @pl.when(i == 0)
    def _():
        place(0, 128, lo[0:128, :])
        place(128, 1024, kv[...])
        place(1152, 128, hi[0:128, :])

    count = SPAN // BLOCK
    starts = [pl.multiple_of(i * SPAN + BLOCK * k, BLOCK) for k in range(count)]
    items = [(k, g, j) for k in range(count) for g in range(2) for j in range(2)]
    for n, (k, g, j) in enumerate(items):
        base = 256 * g + 128 * j
        tile = q[BLOCK * k : BLOCK * (k + 1), base : base + 128]
        zero = jnp.zeros_like(tile)
        both = jnp.concatenate(
            [jnp.where(low_lane, tile, zero), jnp.where(low_lane, zero, tile)], axis=0
        )
        score[n] = dot_rt(keys[g, pl.ds(starts[k], 384), :], both)
    key = iota((128, 128), 0)
    query = iota((128, 128), 1)
    biases = []
    for k in range(count):
        b = i * count + k
        no_left = (b == 0) & (sp == 0)
        no_right = (b == 7) & (sp == lax.axis_size("sp") - 1)
        left_from = jnp.where(no_left, 128, 0)
        right_to = jnp.where(no_right, -1, 127)
        left = jnp.where((key >= query) & (key >= left_from), 0.0, -1e30)
        right = jnp.where((key <= query) & (key <= right_to), 0.0, -1e30)
        biases.append((left, right))
    sinks = []
    for n, (k, g, j) in enumerate(items):
        left, right = biases[k]
        for half in range(2):
            lanes = slice(128 * half, 128 * (half + 1))
            sink_h = jnp.full((1, 128), sink[4 * g + 2 * j + half] * LOG2E, f32)
            low = score[n, 0:128, lanes] + left
            middle = score[n, 128:256, lanes]
            high = score[n, 256:384, lanes] + right
            highest = jnp.max(jnp.maximum(jnp.maximum(low, middle), high), axis=0, keepdims=True)
            highest = jnp.maximum(highest, sink_h)
            weight[n, 0:128, lanes] = jnp.exp2(low - highest).astype(bf16)
            weight[n, 128:256, lanes] = jnp.exp2(middle - highest).astype(bf16)
            weight[n, 256:384, lanes] = jnp.exp2(high - highest).astype(bf16)
            sinks.append(jnp.exp2(sink_h - highest))
    results = [
        dot(vals[g, :, pl.ds(starts[k], 384)], weight[n]) for n, (k, g, j) in enumerate(items)
    ]
    for n, (k, g, j) in enumerate(items):
        finals = []
        for half in range(2):
            lanes = slice(128 * half, 128 * (half + 1))
            denominator = results[n][HEAD : HEAD + 1, lanes] + sinks[2 * n + half]
            finals.append(results[n][0:HEAD, lanes] * (1.0 / denominator))
        base = 256 * g + 128 * j
        out[BLOCK * k : BLOCK * (k + 1), base : base + 128] = (
            jnp.concatenate(finals, axis=0).T.astype(bf16)
        )


def finish_kernel(arrived, add, tot, within, cmat, gate, col, expand, gain, out, entering, made):
    i = pl.program_id(0)

    @pl.when(i == 0)
    def _():
        for c in range(4):
            cols = slice(128 * c, 128 * (c + 1))
            cols_b = slice(512 + 128 * c, 512 + 128 * (c + 1))
            both = [arrived[j, :, cols].astype(f32) for j in range(16)]
            state = jnp.concatenate([slab[0:8] for slab in both], axis=0)
            for b in range(8):
                entering[b, :, cols] = state.astype(bf16)
                if b < 7:
                    state = tot[b : b + 1, cols] * state + add[b, 0, :, cols].astype(f32)
            state = jnp.concatenate([slab[8:16] for slab in both], axis=0)
            for b in reversed(range(8)):
                entering[b, :, cols_b] = state.astype(bf16)
                if b > 0:
                    state = tot[b : b + 1, cols_b] * state + add[b, 1, :, cols].astype(f32)

    count = SPAN // BLOCK
    for k in range(count):
        span = slice(BLOCK * k, BLOCK * (k + 1))
        for g in range(2):
            for d in range(2):
                cols = slice(512 * d + 256 * g, 512 * d + 256 * (g + 1))
                made[span, cols] = dot(
                    cmat[span, 128 * g : 128 * (g + 1)], entering[i * count + k, :, cols]
                )
    for k in range(count):
        span = slice(BLOCK * k, BLOCK * (k + 1))
        widened = dot(col[span, :].astype(bf16), expand[:, 1024:2048])
        for g in range(2):
            cols = slice(256 * g, 256 * (g + 1))
            cols_b = slice(512 + 256 * g, 512 + 256 * (g + 1))
            total = within[span, cols] + widened[:, cols] * made[span, cols]
            total = total + widened[:, cols_b] * made[span, cols_b]
            gates = gate[span, cols].astype(f32)
            gated = total * (gates / (1.0 + jnp.exp(-gates)))
            mean = jnp.mean(gated * gated, axis=1, keepdims=True)
            out[span, cols] = (gated * lax.rsqrt(mean + EPS) * gain[:, cols]).astype(bf16)


def output_kernel(attn, mixed, wa, ws, out, *, swapped):
    t = lax.axis_index("tp")
    half = 1 - t if swapped else t
    rows = pl.ds(pl.multiple_of(half * ROWS, ROWS), ROWS)
    out[...] = (dot(attn[rows, :], wa[...]) + dot(mixed[rows, :], ws[...])).astype(bf16)


def call(kernel, name, grid, in_specs, out_specs, out_shape, scratch=(), flops=0, nbytes=0, mib=40):
    return pl.pallas_call(
        kernel,
        name=name,
        grid_spec=pltpu.PrefetchScalarGridSpec(
            num_scalar_prefetch=0,
            grid=grid,
            in_specs=in_specs,
            out_specs=out_specs,
            scratch_shapes=list(scratch),
        ),
        out_shape=out_shape,
        cost_estimate=pl.CostEstimate(flops=flops, transcendentals=0, bytes_accessed=nbytes),
        compiler_params=pltpu.CompilerParams(
            dimension_semantics=("arbitrary",) * len(grid), vmem_limit_bytes=mib << 20
        ),
    )


def local(
    inputs, mix_gain, w_query, w_key, w_value, query_gain, key_gain, sink_logit, w_inner, w_bmat,
    w_cmat, w_gate, w_step, conv_inner, conv_bmat, conv_cmat, step_bias, decay_rate, decay_offset,
    start_state, group_gain, w_out_attn, w_out_state,
):
    sp_count = lax.axis_size("sp")
    swap = [(0, 1), (1, 0)]
    other = lax.ppermute(inputs, "tp", swap)

    cosb, sinb = rotation_tables(np.arange(128) * BLOCK)
    cosi, sini = rotation_tables(np.arange(BLOCK))
    scalar = pl.BlockSpec(memory_space=pltpu.SMEM)
    rows2 = lambda width: pl.BlockSpec((ROWS, width), lambda i: (i, 0))
    grid = (1024 // ROWS,)
    step_w = w_step.transpose(1, 2, 0).reshape(16, D)
    widths = (512, 256, 512, 256, 256, 512)
    any_space = pl.BlockSpec(memory_space=pl.ANY)
    part = lambda width: pl.BlockSpec((PART, width), lambda i: (i, 0))
    early = call(
        early_kernel, "early", (1024 // PART,),
        [part(HALF), once((1, D))] + [any_space] * 7 + [once((16, D))],
        [VM] * 14,
        [vmem((1024, 128), f32)]
        + [vmem((1024, width), f32) for width in widths] + [vmem((1024, 16), f32)]
        + [vmem((HALF, width), bf16) for width in widths],
        scratch=[pltpu.VMEM((HALF, width), bf16) for width in widths]
        + [pltpu.VMEM((PART, HALF), bf16), pltpu.SemaphoreType.DMA((14,))],
        flops=1024 * D * 2320, nbytes=20 << 20, mib=20,
    )(
        far(inputs), far(mix_gain.reshape(1, D)), far(w_query), far(w_key), far(w_value),
        far(w_inner), far(w_bmat), far(w_cmat), far(w_gate), far(step_w),
    )
    queries, kv, p1, pc, step_t, gate, lo_edge, hi_edge = call(
        project_kernel, "project", grid,
        [
            VM, once((1, D)), once((16, D)), once((1, 64)), once((128, 128)), once((128, 128)),
            once((128, 128)), once((128, 128)),
        ]
        + [VM] * 14,
        [
            VM, rows2(256), VM, rows2(256), pl.BlockSpec((16, ROWS), lambda i: (0, i)),
            rows2(512), whole((192, 256)), whole((192, 256)),
        ],
        [
            vmem((1024, 512), bf16), hbm((1024, 256), bf16), vmem((1024, 768), bf16),
            hbm((1024, 256), bf16), hbm((16, 1024), f32), hbm((1024, 512), bf16), sds((192, 256), bf16),
            sds((192, 256), bf16),
        ],
        scratch=[
            pltpu.VMEM((1, ROWS, 128), f32), pltpu.VMEM((1, ROWS, 128), bf16),
            pltpu.VMEM((ROWS, HALF), bf16),
        ],
        flops=1024 * D * 2320, nbytes=20 << 20, mib=28,
    )(
        near(other), far(mix_gain.reshape(1, D)), far(step_w), far(key_gain.reshape(1, HEAD)),
        far(cosb), far(sinb), far(cosi), far(sini), *[near(value) for value in early],
    )

    forward = [(i, i + 1) for i in range(sp_count - 1)]
    backward = [(i + 1, i) for i in range(sp_count - 1)]
    lo = lax.ppermute(hi_edge, "sp", forward)
    hi = lax.ppermute(lo_edge, "sp", backward)

    rows, col, q_rot = call(
        steps_kernel, "steps", (1,),
        [whole((16, 1024)), scalar, scalar, whole((16, 1024)), VM, whole((1, 64))]
        + [whole((128, 128))] * 4,
        [whole((8, 24, 128)), whole((1024, 128)), whole((1024, 512))],
        [hbm((8, 24, 128), f32), hbm((1024, 128), f32), hbm((1024, 512), bf16)],
        scratch=[pltpu.VMEM((4, 1024, 128), f32), pltpu.VMEM((4, 1024, 128), bf16)],
        flops=1 << 28, nbytes=3 << 20,
    )(
        far(step_t), step_bias, decay_rate, far(decay_offset.reshape(1024, 16).T), near(queries),
        far(query_gain.reshape(1, HEAD)), far(cosb), far(sinb), far(cosi), far(sini),
    )

    lane = np.arange(1024)
    unit = lane // HEAD
    expand = np.zeros((128, 2048), np.float32)
    for u in range(16):
        for base, shift in ((16, 0), (32, 0), (48, 1024), (64, 1024)):
            expand[base + u, shift : shift + 1024] = unit == u
    expand = jnp.asarray(expand, bf16)
    pick = np.zeros((1536, 128), np.float32)
    for third in range(3):
        for h in range(HEADS):
            pick[512 * third + HEAD * h, 8 * third + h] = 1
    pick = jnp.asarray(pick, bf16)
    spread = np.zeros((128, 512), np.float32)
    for j in range(24):
        spread[j] = (lane[:512] // HEAD) == (j % 8)
    spread = jnp.asarray(spread, bf16)

    count = SPAN // BLOCK
    blocks = (1024 // SPAN,)
    rows1 = lambda width: pl.BlockSpec((SPAN, width), lambda b: (b, 0))
    inner, bmat, add, tot, pack = call(
        mixer_kernel, "mixer", blocks,
        [
            VM, VM, VM, once((CONV, 512)), once((CONV, 256)), rows1(128), once((128, 2048)),
            once((1536, 128)),
        ],
        [
            rows1(512), rows1(256), pl.BlockSpec((count, 2, 128, 512), lambda b: (b, 0, 0, 0)),
            whole((8, 1024)), whole((16, 16, 640)),
        ],
        [
            hbm((1024, 512), bf16), hbm((1024, 256), bf16), hbm((8, 2, 128, 512), bf16),
            hbm((8, 1024), f32), sds((16, 16, 640), bf16),
        ],
        scratch=[
            pltpu.VMEM((6, SPAN + 16, 128), f32), pltpu.VMEM((128, 512), f32),
            pltpu.VMEM((128, 512), f32), pltpu.VMEM((1, 512), f32), pltpu.VMEM((1, 512), f32),
            pltpu.VMEM((SPAN, 1024), bf16), pltpu.VMEM((count, 2, 128, 512), f32),
        ],
        flops=1 << 30, nbytes=12 << 20,
    )(near(p1), near(lo), near(hi), conv_inner, conv_bmat, far(col), far(expand), far(pick))

    arrived = lax.all_to_all(pack, "sp", 0, 0, tiled=True)
    attention = call(
        attend_kernel, "attend", blocks,
        [rows1(512), once((1024, 256)), VM, VM, scalar], rows1(512), hbm((1024, 512), bf16),
        scratch=[
            pltpu.VMEM((2, 1280, 128), bf16), pltpu.VMEM((2, 128, 1280), bf16),
            pltpu.VMEM((4 * count, 384, 256), f32), pltpu.VMEM((4 * count, 384, 256), bf16),
        ],
        flops=1 << 31, nbytes=4 << 20,
    )(far(q_rot), far(kv), near(lo), near(hi), sink_logit)
    start_t = start_state.reshape(2, 512, 16, 8).transpose(0, 2, 3, 1)
    arrived, attention, start_t = lax.optimization_barrier((arrived, attention, start_t))
    carried = call(
        carry_kernel, "carry", (1,), [VM, whole((2, 16, 8, 512)), whole((128, 512))],
        whole((16, 16, 512)), sds((16, 16, 512), bf16),
        scratch=[pltpu.VMEM((16, 16, 512), f32), pltpu.VMEM((16, 16, 512), f32)],
        flops=1 << 22, nbytes=1 << 20,
    )(near(arrived), start_t, far(spread))
    carried, pc, inner, bmat = lax.optimization_barrier((carried, pc, inner, bmat))
    returned = lax.all_to_all(carried, "sp", 0, 0, tiled=True)
    within, cmat = call(
        within_kernel, "within", blocks,
        [
            once((1024, 256)), VM, VM, once((CONV, 256)),
            pl.BlockSpec((count, 24, 128), lambda b: (b, 0, 0)), rows1(128), rows1(512), rows1(256),
        ],
        [rows1(512), rows1(256)], [hbm((1024, 512), f32), hbm((1024, 256), bf16)],
        scratch=[
            pltpu.VMEM((2, SPAN + 16, 128), f32), pltpu.VMEM((count, 2, 128, 128), f32),
            pltpu.VMEM((count, 4, 128, 256), bf16),
        ],
        flops=1 << 30, nbytes=8 << 20,
    )(far(pc), near(lo), near(hi), far(conv_cmat), far(rows), far(col), far(inner), far(bmat))
    returned, within, cmat = lax.optimization_barrier((returned, within, cmat))
    state_out = call(
        finish_kernel, "finish", blocks,
        [
            VM, once((8, 2, 128, 512)), once((8, 1024)), rows1(512), rows1(256), rows1(512),
            rows1(128), once((128, 2048)), once((1, 512)),
        ],
        rows1(512), sds((1024, 512), bf16),
        scratch=[pltpu.VMEM((8, 128, 1024), bf16), pltpu.VMEM((SPAN, 1024), f32)],
        flops=1 << 29, nbytes=10 << 20, mib=24,
    )(
        near(returned), far(add), far(tot), far(within), far(cmat), far(gate), far(col),
        far(expand), group_gain.reshape(1, 512),
    )

    def projected(swapped):
        weight = pl.BlockSpec((512, 512), lambda n: (0, n))
        return call(
            functools.partial(output_kernel, swapped=swapped), "output", (4,),
            [once((1024, 512)), once((1024, 512)), weight, weight],
            pl.BlockSpec((ROWS, 512), lambda n: (0, n)), sds((ROWS, D), bf16),
            flops=2 * 512 * 1024 * D, nbytes=8 << 20, mib=16,
        )(attention, state_out, w_out_attn, w_out_state)

    sent = projected(True)
    received = lax.ppermute(sent, "tp", swap)
    kept = projected(False)
    return (kept.astype(f32) + received.astype(f32)).astype(bf16)


def solution(mesh):
    return jax.shard_map(
        local,
        mesh=mesh,
        in_specs=(
            P(("fs", "sp"), "tp"), P(), P(None, "tp"), P(None, "tp"), P(None, "tp"), P(), P(),
            P("tp"), P(None, "tp"), P(None, "tp"), P(None, "tp"), P(None, "tp"),
            P(None, None, "tp"), P(None, "tp"), P(None, "tp"), P(None, "tp"), P(None, "tp"),
            P(None, "tp"), P("sp", None, "tp"), P("fs", "tp", None, None), P("tp"),
            P("tp", None), P("tp", None),
        ),
        out_specs=P(("fs", "sp", "tp"), None),
        check_vma=False,
    )
```

```python
import functools

import jax
import jax.numpy as jnp
import numpy as np
from jax import lax
from jax.experimental import pallas as pl
from jax.experimental.pallas import tpu as pltpu
from jax.sharding import PartitionSpec as P

D = 2048
HALF = 1024
HEAD = 64
STATE = 128
CONV = 5
BLOCK = 128
EPS = 1e-06
BASE = 10000.0
HEADS = 8
LOG2E = 1.4426950408889634
ROWS = 512
PART = 512
SPAN = 256
ASPAN = 512
MSPAN = 256
PROWS = 1024
FSPAN = 512
f32 = jnp.float32
bf16 = jnp.bfloat16


def dot(a, b):
    return jnp.dot(a, b, preferred_element_type=f32)


def dot_rt(a, b):
    return lax.dot_general(a, b, (((1,), (1,)), ((), ())), preferred_element_type=f32)


def split2(v):
    hi = v.astype(bf16).astype(f32)
    return hi, (v - hi).astype(bf16).astype(f32)


def split3(v):
    hi = v.astype(bf16).astype(f32)
    rest = v - hi
    mid = rest.astype(bf16).astype(f32)
    return hi, mid, (rest - mid).astype(bf16).astype(f32)


def iota(shape, dim):
    return lax.broadcasted_iota(jnp.int32, shape, dim)


def whole(shape):
    zeros = (0,) * len(shape)
    return pl.BlockSpec(shape, lambda *_: zeros)


def once(shape):
    zeros = (0,) * len(shape)
    return pl.BlockSpec(shape, lambda *_: zeros, pipeline_mode=pl.Buffered(1))


def near(value):
    return pltpu.with_memory_space_constraint(value, pltpu.VMEM)


def far(value):
    return pltpu.with_memory_space_constraint(value, pltpu.HBM)


VM = pl.BlockSpec(memory_space=pltpu.VMEM)


def hbm(shape, dtype):
    return pltpu.HBM(shape, dtype)


def vmem(shape, dtype):
    return pltpu.VMEM(shape, dtype)


def sds(shape, dtype):
    return jax.ShapeDtypeStruct(shape, dtype)


def rotation_tables(positions):
    lane = np.arange(128) % 32
    freq = BASE ** (-lane.astype(np.float64) / 32)
    angles = positions.astype(np.float64)[:, None] * freq[None, :]
    return np.cos(angles).astype(np.float32), np.sin(angles).astype(np.float32)


def early_kernel(
    xo, gain, wq, wk, wv, wi, wb, wc, wg, ws,
    ss_o, aq, akv, ai, ab, ac, ag, at, pq, pkv, pi, pb, pc, pg,
    oq, okv, oi, ob, oc, og, xs_o, sems,
):
    i = pl.program_id(0)
    t = lax.axis_index("tp")
    own = pl.multiple_of(t * HALF, HALF)
    peer = pl.multiple_of((1 - t) * HALF, HALF)

    def copies(first, targets, base):
        q, kv, inner, bm, cm, gm = targets
        pairs = (
            (wq, q), (wk, kv.at[:, 0:128]), (wv, kv.at[:, 128:256]), (wi, inner), (wb, bm),
            (wc, cm), (wg, gm),
        )
        return [
            pltpu.make_async_copy(w.at[pl.ds(first, HALF), :], target, sems.at[base + n])
            for n, (w, target) in enumerate(pairs)
        ]

    mine = copies(own, (oq, okv, oi, ob, oc, og), 0)
    others = copies(peer, (pq, pkv, pi, pb, pc, pg), 7)

    @pl.when(i == 0)
    def _():
        for copy in mine:
            copy.start()

    own_x = xo[...].astype(f32)
    rows = pl.ds(pl.multiple_of(i * PART, PART), PART)
    xs_o[...] = (own_x * gain[:, pl.ds(own, HALF)]).astype(bf16)
    ss_o[rows, :] = jnp.broadcast_to(jnp.sum(own_x * own_x, axis=1, keepdims=True), (PART, 128))

    @pl.when(i == 0)
    def _():
        for copy in mine:
            copy.wait()

    for w, acc in ((oq, aq), (okv, akv), (oi, ai), (ob, ab), (oc, ac), (og, ag)):
        acc[rows, :] = dot(xs_o[...], w[...])
    at[rows, :] = dot_rt(xs_o[...], ws[:, pl.ds(own, HALF)])

    @pl.when(i == 0)
    def _():
        for copy in others:
            copy.start()

    @pl.when(i == pl.num_programs(0) - 1)
    def _():
        for copy in others:
            copy.wait()


def swapped(value):
    first = (iota((1, 128), 1) % HEAD) < (HEAD // 2)
    return jnp.where(first, pltpu.roll(value, 96, 1), pltpu.roll(value, 32, 1))


def norm_and_rotate(tiles, outs, gain, first_block, tables, means, scaled):
    cosb, sinb, cosi, sini = tables
    same = (iota((128, 128), 0) // HEAD) == (iota((128, 128), 1) // HEAD)
    averaging = jnp.where(same, 1.0 / HEAD, 0.0).astype(bf16)
    for j, tile in enumerate(tiles):
        values = tile[...].astype(f32)
        scaled[j] = (values * values).astype(bf16)
    for j in range(len(tiles)):
        means[j] = dot(scaled[j], averaging)
    first = (iota((1, 128), 1) % HEAD) < (HEAD // 2)
    wide = jnp.broadcast_to(jnp.concatenate([gain, gain], axis=1), (8, 128))
    gain_a, gain_b = wide[0:1], swapped(wide)[0:1]
    for s in range(tiles[0].shape[0] // BLOCK):
        span = slice(BLOCK * s, BLOCK * (s + 1))
        cb = cosb[pl.ds(first_block + s, 1), :]
        sb = sinb[pl.ds(first_block + s, 1), :]
        cosine = (cb * cosi[...] - sb * sini[...]) * gain_a
        sine = (sb * cosi[...] + cb * sini[...]) * gain_b
        sine = jnp.where(first, -sine, sine)
        for j, tile in enumerate(tiles):
            y = tile[span, :].astype(f32)
            y = (y * cosine + swapped(y) * sine) * lax.rsqrt(means[j, span, :] + EPS)
            outs[j][span, :] = y.astype(bf16)


def project_kernel(
    xp, gain, ws, kg, cosb, sinb, cosi, sini,
    ss, aq, akv, ai, ab, ac, ag, at, wq, wkv, wi, wb, wc, wg,
    q_o, kv_o, p1_o, pc_o, st_o, gate_o, lo_o, hi_o, means, scaled, xs_o,
):
    i = pl.program_id(0)
    t = lax.axis_index("tp")
    sp = lax.axis_index("sp")
    peer = pl.multiple_of((1 - t) * HALF, HALF)
    rows = pl.ds(pl.multiple_of(i * PROWS, PROWS), PROWS)
    peer_x = xp[rows, :].astype(f32)
    xs_o[...] = (peer_x * gain[:, pl.ds(peer, HALF)]).astype(bf16)
    squares = ss[rows, 0:1] + jnp.sum(peer_x * peer_x, axis=1, keepdims=True)
    rs = lax.rsqrt(squares * (1.0 / D) + EPS)

    def proj(w, acc):
        return (dot(xs_o[...], w[...]) + acc[rows, :]) * rs

    kv_o[...] = proj(wkv, akv).astype(bf16)
    p1_o[rows, 0:512] = proj(wi, ai).astype(bf16)
    tile = [kv_o.at[:, 0:128]]
    p1_o[rows, 512:768] = proj(wb, ab).astype(bf16)
    pc_o[...] = proj(wc, ac).astype(bf16)
    q_o[rows, :] = proj(wq, aq).astype(bf16)
    gate_o[...] = proj(wg, ag).astype(bf16)
    block = sp * 8 + i * (PROWS // BLOCK)
    norm_and_rotate(tile, tile, kg[...], block, (cosb, sinb, cosi, sini), means, scaled)
    steps = (dot_rt(xs_o[...], ws[:, pl.ds(peer, HALF)]) + at[rows, :]) * rs
    st_o[...] = jnp.concatenate([steps, jnp.zeros((PROWS, 112), f32)], axis=1).T[0:16, :]

    @pl.when(i == 0)
    def _():
        lo_o[0:128, :] = kv_o[0:128, :]
        for j in range(3):
            lo_o[128 + 16 * j : 144 + 16 * j, :] = p1_o[0:16, 256 * j : 256 * (j + 1)]
        lo_o[176:192, :] = pc_o[0:16, :]

    @pl.when(i == pl.num_programs(0) - 1)
    def _():
        hi_o[0:128, :] = kv_o[PROWS - 128 : PROWS, :]
        for j in range(3):
            hi_o[128 + 16 * j : 144 + 16 * j, :] = p1_o[
                1024 - 16 : 1024, 256 * j : 256 * (j + 1)
            ]
        hi_o[176:192, :] = pc_o[PROWS - 16 : PROWS, :]


def steps_kernel(
    st, bias, rate, offset, q, qg, cosb, sinb, cosi, sini, rows_o, col_o, q_o, means, scaled
):
    tiles = [q.at[:, 128 * j : 128 * (j + 1)] for j in range(4)]
    outs = [q_o.at[:, 128 * j : 128 * (j + 1)] for j in range(4)]
    gain = qg[...] * (HEAD**-0.5 * LOG2E)
    first_block = lax.axis_index("sp") * 8
    norm_and_rotate(tiles, outs, gain, first_block, (cosb, sinb, cosi, sini), means, scaled)
    unit = iota((16, 1), 0)

    def as_column(table):
        value = jnp.zeros((16, 1), f32)
        for d in range(2):
            for h in range(HEADS):
                value = jnp.where(unit == 8 * d + h, table[d, h], value)
        return value

    v = st[...] + as_column(bias)
    step = jnp.maximum(v, 0.0) + jnp.log1p(jnp.exp(-jnp.abs(v)))
    decay = -as_column(rate) * step + offset[...]
    count = 1024 // BLOCK
    parts = [decay[:, BLOCK * s : BLOCK * (s + 1)] for s in range(count)]
    stacked = jnp.concatenate(parts, axis=0)
    hi, mid, lo = split3(stacked)
    row = iota((128, 256), 0)
    column = iota((128, 256), 1)
    prefix = (column < 128) & (row <= column)
    suffix = (column >= 128) & (row >= column - 128)
    sums = jnp.where(prefix | suffix, 1.0, 0.0).astype(bf16)
    total = dot(hi.astype(bf16), sums) + dot(mid.astype(bf16), sums) + dot(lo.astype(bf16), sums)
    for s in range(count):
        c = jnp.concatenate(
            [total[16 * s : 16 * s + 8, 0:128], total[16 * s + 8 : 16 * s + 16, 128:256]], axis=0
        )
        steps = step[:, BLOCK * s : BLOCK * (s + 1)]
        last = jnp.concatenate([c[0:8, 127:128], c[8:16, 0:1]], axis=0)
        factor = steps * jnp.exp(last - c)
        raised = jnp.exp(c)
        rows_o[s, 0:16, :] = (jnp.log(steps) - c) * LOG2E
        rows_o[s, 16:24, :] = steps[0:8] + steps[8:16]
        factor_hi, factor_lo = split2(factor)
        raised_hi, raised_lo = split2(raised)
        packed = jnp.concatenate(
            [c * LOG2E, factor_hi, factor_lo, raised_hi, raised_lo, jnp.zeros((48, 128), f32)],
            axis=0,
        )
        col_o[BLOCK * s : BLOCK * (s + 1), :] = packed.T


def frame(p1, lo, hi, xpad, first_piece):
    i = pl.program_id(0)
    rows = xpad.shape[1] - 16
    start = pl.multiple_of(i * rows, rows)
    final = pl.num_programs(0) - 1
    chunks = xpad.shape[0]
    after_rows = slice(rows + 8, rows + 16)

    @pl.when(i == 0)
    def _():
        for c in range(chunks):
            top = 128 + 16 * (first_piece + c // 2)
            lanes = slice(128 * (c % 2), 128 * (c % 2) + 128)
            xpad[c, 0:8, :] = lo[top : top + 16, lanes].astype(f32)[8:16]

    @pl.when(i > 0)
    def _():
        before = pl.multiple_of(jnp.maximum(start - 16, 0), 16)
        rim = p1[pl.ds(before, 16), :].astype(f32)[8:16]
        for c in range(chunks):
            xpad[c, 0:8, :] = rim[:, 128 * c : 128 * (c + 1)]

    @pl.when(i < final)
    def _():
        after = pl.multiple_of(jnp.minimum(start + rows, 1008), 16)
        rim = p1[pl.ds(after, 16), :].astype(f32)[0:8]
        for c in range(chunks):
            xpad[c, after_rows, :] = rim[:, 128 * c : 128 * (c + 1)]

    @pl.when(i == final)
    def _():
        for c in range(chunks):
            top = 128 + 16 * (first_piece + c // 2)
            lanes = slice(128 * (c % 2), 128 * (c % 2) + 128)
            xpad[c, after_rows, :] = hi[top : top + 16, lanes].astype(f32)[0:8]

    for c in range(chunks):
        xpad[c, 8 : rows + 8, :] = p1[pl.ds(start, rows), 128 * c : 128 * (c + 1)].astype(f32)


def convolve(xpad, taps, chunk, out):
    table = taps[...].astype(f32)
    rows = xpad.shape[1] - 16
    for c in range(taps.shape[1] // 128):
        lanes = slice(128 * c, 128 * (c + 1))
        total = table[0:1, lanes] * xpad[chunk + c, 6 : 6 + rows, :]
        for j in range(1, CONV):
            total = total + table[j : j + 1, lanes] * xpad[chunk + c, 6 + j : 6 + j + rows, :]
        out[:, lanes] = (total / (1.0 + jnp.exp(-total))).astype(bf16)


def mixer_kernel(
    p1, lo, hi, ti, tb, col, expand,
    inner_s, bs, add_o, tot_o, pack_o,
    xpad, run_f, run_b, prod_f, prod_b, loaded, added,
):
    i = pl.program_id(0)

    @pl.when(i == 0)
    def _():
        run_f[...] = jnp.zeros_like(run_f)
        run_b[...] = jnp.zeros_like(run_b)
        prod_f[...] = jnp.ones_like(prod_f)
        prod_b[...] = jnp.ones_like(prod_b)

    frame(p1, lo, hi, xpad, 0)
    count = MSPAN // BLOCK
    spans = [slice(BLOCK * k, BLOCK * (k + 1)) for k in range(count)]
    groups = [slice(128 * g, 128 * (g + 1)) for g in range(2)]
    convolve(xpad, tb, 4, bs)
    flipped = bs[...].astype(f32).T.astype(bf16)
    convolve(xpad, ti, 0, inner_s)
    factors = col[...].astype(bf16)
    tot_f, tot_b = [], []
    for k in range(count):
        widened = dot(factors[spans[k], :], expand[:, 0:1024])
        end = dot(factors[BLOCK * k + 112 : BLOCK * k + 128, :], expand[:, 1024:1536])
        begin = dot(factors[BLOCK * k : BLOCK * k + 16, :], expand[:, 1536:2048])
        inner_wide = inner_s[spans[k], :].astype(f32)
        loaded[spans[k], 0:512] = (inner_wide * widened[:, 0:512]).astype(bf16)
        loaded[spans[k], 512:1024] = (inner_wide * widened[:, 512:1024]).astype(bf16)
        tot_f.append(end[15:16])
        tot_b.append(begin[0:1])
        tot_o[pl.ds(i * count + k, 1), 0:512] = tot_f[k]
        tot_o[pl.ds(i * count + k, 1), 512:1024] = tot_b[k]
    for k in range(count):
        for g in range(2):
            for d in range(2):
                cols = slice(256 * g, 256 * (g + 1))
                cols_d = slice(512 * d + 256 * g, 512 * d + 256 * (g + 1))
                added[k, d, :, cols] = dot(flipped[groups[g], spans[k]], loaded[spans[k], cols_d])
    for k in range(count):
        for c in range(4):
            cols = slice(128 * c, 128 * (c + 1))
            run_f[:, cols] = tot_f[k][:, cols] * run_f[:, cols] + added[k, 0, :, cols]
            run_b[:, cols] = run_b[:, cols] + prod_b[:, cols] * added[k, 1, :, cols]
        add_o[k] = added[k].astype(bf16)
        prod_f[...] = prod_f[...] * tot_f[k]
        prod_b[...] = prod_b[...] * tot_b[k]

    @pl.when(i == pl.num_programs(0) - 1)
    def _():
        levels = jnp.concatenate([prod_f[...], prod_b[...]], axis=0)
        hi_l, mid_l, lo_l = split3(levels)
        joined = jnp.concatenate([hi_l, mid_l, lo_l], axis=1).astype(bf16)
        lane = iota((1536, 128), 0)
        head = iota((1536, 128), 1)
        wanted = (lane // 512) * 8 + (lane % 512) // HEAD
        pick = jnp.where((lane % HEAD == 0) & (head == wanted), 1.0, 0.0).astype(bf16)
        sent = dot(joined, pick)
        sent = jnp.concatenate(
            [jnp.broadcast_to(sent[0:1], (8, 128)), jnp.broadcast_to(sent[1:2], (8, 128))], axis=0
        ).astype(bf16)
        for j in range(16):
            pack_o[j, :, 0:512] = jnp.concatenate(
                [run_f[8 * j : 8 * j + 8, :], run_b[8 * j : 8 * j + 8, :]], axis=0
            ).astype(bf16)
            pack_o[j, :, 512:640] = sent


def within_kernel(
    pc, lo, hi, tc, rows, col, inner, bmat, add, tot, expand,
    within_o, cmat_o, xpad, score, weight, begun, made,
):
    i = pl.program_id(0)

    @pl.when(i == 0)
    def _():
        for d in range(2):
            for c in range(4):
                cols = slice(128 * c, 128 * (c + 1))
                cols_d = slice(512 * d + 128 * c, 512 * d + 128 * (c + 1))
                state = jnp.zeros((128, 128), f32)
                for b in range(8) if d == 0 else reversed(range(8)):
                    begun[b, :, cols_d] = state.astype(bf16)
                    if b != (7 if d == 0 else 0):
                        state = tot[b : b + 1, cols_d] * state + add[b, d, :, cols].astype(f32)

    frame(pc, lo, hi, xpad, 3)
    convolve(xpad, tc, 0, cmat_o)
    count = SPAN // BLOCK
    spans = [slice(BLOCK * k, BLOCK * (k + 1)) for k in range(count)]
    groups = [slice(128 * g, 128 * (g + 1)) for g in range(2)]
    for k in range(count):
        for g in range(2):
            score[k, g] = dot_rt(cmat_o[spans[k], groups[g]], bmat[spans[k], groups[g]])

    @pl.when(i >= 0)
    def _():
        for k in range(count):
            for g in range(2):
                for d in range(2):
                    cols = slice(512 * d + 256 * g, 512 * d + 256 * (g + 1))
                    made[spans[k], cols] = dot(
                        cmat_o[spans[k], groups[g]], begun[i * count + k, :, cols]
                    )
        for k in range(count):
            widened = dot(col[spans[k], :].astype(bf16), expand[...])
            within_o[spans[k], :] = (
                widened[:, 0:512] * made[spans[k], 0:512]
                + widened[:, 512:1024] * made[spans[k], 512:1024]
            )

    row = iota((128, 128), 0)
    column = iota((128, 128), 1)
    causal = row >= column
    diagonal = row == column
    for k in range(count):
        for h in range(HEADS):
            forward = col[spans[k], h : h + 1] + rows[k, h : h + 1, :]
            backward = col[spans[k], 8 + h : 9 + h] + rows[k, 8 + h : 9 + h, :]
            spread = jnp.exp2(jnp.where(causal, forward, backward))
            spread = jnp.where(diagonal, rows[k, 16 + h : 17 + h, :], spread)
            weight[k, h // 2, :, 128 * (h % 2) : 128 * (h % 2) + 128] = (
                score[k, h // 4] * spread
            ).astype(bf16)
    low_lane = iota((1, 128), 1) < HEAD
    for k in range(count):
        for pair in range(HEADS // 2):
            both = inner[spans[k], 128 * pair : 128 * (pair + 1)]
            zero = jnp.zeros_like(both)
            right = jnp.concatenate(
                [jnp.where(low_lane, both, zero), jnp.where(low_lane, zero, both)], axis=0
            )
            cols = slice(128 * pair, 128 * (pair + 1))
            within_o[spans[k], cols] = within_o[spans[k], cols] + dot(weight[k, pair], right)


def carry_kernel(arrived, start, out, wide, held, first, sem):
    fetch = pltpu.make_async_copy(start.at[:, lax.axis_index("sp")], first, sem)
    fetch.start()
    lane = iota((128, 512), 0)
    spread = (lane < 24) & (iota((128, 512), 1) // HEAD == lane % 8)
    spread = jnp.where(spread, 1.0, 0.0).astype(bf16)
    for j in range(16):
        wide[j] = dot(arrived[j, :, 512:640], spread)
    fetch.wait()
    state = first[0]
    for j in range(16):
        held[j, 0:8, :] = state
        state = wide[j, 0:8, :] * state + arrived[j, :, 0:512].astype(f32)[0:8]
    state = first[1]
    for j in reversed(range(16)):
        held[j, 8:16, :] = state
        state = wide[j, 8:16, :] * state + arrived[j, :, 0:512].astype(f32)[8:16]
    for j in range(16):
        out[j] = held[j].astype(bf16)


def attend_kernel(q, kv, lo, hi, sink, out, keys, vals, score, weight):
    i = pl.program_id(0)
    sp = lax.axis_index("sp")
    low_lane = iota((1, 128), 1) < HEAD

    def place(first, count, pairs):
        kk = pairs[:, 0:128].astype(f32)
        kr = pltpu.roll(kk, 64, 1)
        span = slice(first, first + count)
        keys[0, span, :] = jnp.where(low_lane, kk, kr).astype(bf16)
        keys[1, span, :] = jnp.where(low_lane, kr, kk).astype(bf16)
        flipped = pairs[:, 128:256].astype(f32).T.astype(bf16)
        ones = jnp.ones((HEAD, count), bf16)
        for g in range(2):
            vals[g, 0:HEAD, span] = flipped[HEAD * g : HEAD * (g + 1)]
            vals[g, HEAD:128, span] = ones

    @pl.when(i == 0)
    def _():
        place(0, 128, lo[0:128, :])
        place(128, 1024, kv[...])
        place(1152, 128, hi[0:128, :])

    count = ASPAN // BLOCK
    starts = [pl.multiple_of(i * ASPAN + BLOCK * k, BLOCK) for k in range(count)]
    items = [(k, g, j) for k in range(count) for g in range(2) for j in range(2)]
    for n, (k, g, j) in enumerate(items):
        base = 256 * g + 128 * j
        tile = q[BLOCK * k : BLOCK * (k + 1), base : base + 128]
        zero = jnp.zeros_like(tile)
        both = jnp.concatenate(
            [jnp.where(low_lane, tile, zero), jnp.where(low_lane, zero, tile)], axis=0
        )
        score[n] = dot_rt(keys[g, pl.ds(starts[k], 384), :], both)
    key = iota((128, 128), 0)
    query = iota((128, 128), 1)
    biases = []
    for k in range(count):
        b = i * count + k
        no_left = (b == 0) & (sp == 0)
        no_right = (b == 7) & (sp == lax.axis_size("sp") - 1)
        left_from = jnp.where(no_left, 128, 0)
        right_to = jnp.where(no_right, -1, 127)
        left = jnp.where((key >= query) & (key >= left_from), 0.0, -1e30)
        right = jnp.where((key <= query) & (key <= right_to), 0.0, -1e30)
        biases.append((left, right))
    sinks = []
    for n, (k, g, j) in enumerate(items):
        left, right = biases[k]
        for half in range(2):
            lanes = slice(128 * half, 128 * (half + 1))
            sink_h = jnp.full((1, 128), sink[4 * g + 2 * j + half] * LOG2E, f32)
            low = score[n, 0:128, lanes] + left
            middle = score[n, 128:256, lanes]
            high = score[n, 256:384, lanes] + right
            highest = jnp.max(jnp.maximum(jnp.maximum(low, middle), high), axis=0, keepdims=True)
            highest = jnp.maximum(highest, sink_h)
            weight[n, 0:128, lanes] = jnp.exp2(low - highest).astype(bf16)
            weight[n, 128:256, lanes] = jnp.exp2(middle - highest).astype(bf16)
            weight[n, 256:384, lanes] = jnp.exp2(high - highest).astype(bf16)
            sinks.append(jnp.exp2(sink_h - highest))
    results = [
        dot(vals[g, :, pl.ds(starts[k], 384)], weight[n]) for n, (k, g, j) in enumerate(items)
    ]
    for n, (k, g, j) in enumerate(items):
        finals = []
        for half in range(2):
            lanes = slice(128 * half, 128 * (half + 1))
            denominator = results[n][HEAD : HEAD + 1, lanes] + sinks[2 * n + half]
            finals.append(results[n][0:HEAD, lanes] * (1.0 / denominator))
        base = 256 * g + 128 * j
        out[BLOCK * k : BLOCK * (k + 1), base : base + 128] = (
            jnp.concatenate(finals, axis=0).T.astype(bf16)
        )


def finish_kernel(arrived, tot, within, cmat, gate, col, expand, gain, out, entering, kept, made):
    i = pl.program_id(0)

    @pl.when(i == 0)
    def _():
        for j in range(16):
            slab = arrived[j].astype(f32)
            made[8 * j : 8 * j + 8, 0:512] = slab[0:8]
            made[8 * j : 8 * j + 8, 512:1024] = slab[8:16]
        entering[...] = made[0:128, :].astype(bf16)
        level = jnp.ones((1, 512), f32)
        for b in range(8):
            kept[b : b + 1, 0:512] = level
            level = level * tot[b : b + 1, 0:512]
        level = jnp.ones((1, 512), f32)
        for b in reversed(range(8)):
            kept[b : b + 1, 512:1024] = level
            level = level * tot[b : b + 1, 512:1024]

    count = FSPAN // BLOCK
    for g in range(2):
        for d in range(2):
            cols = slice(512 * d + 256 * g, 512 * d + 256 * (g + 1))
            made[:, cols] = dot(cmat[:, 128 * g : 128 * (g + 1)], entering[:, cols])
    for k in range(count):
        span = slice(BLOCK * k, BLOCK * (k + 1))
        widened = dot(col[span, :].astype(bf16), expand[...]) * kept[pl.ds(i * count + k, 1), :]
        for g in range(2):
            cols = slice(256 * g, 256 * (g + 1))
            cols_b = slice(512 + 256 * g, 512 + 256 * (g + 1))
            total = within[span, cols] + widened[:, cols] * made[span, cols]
            total = total + widened[:, cols_b] * made[span, cols_b]
            gates = gate[span, cols].astype(f32)
            gated = total * (gates / (1.0 + jnp.exp(-gates)))
            mean = jnp.mean(gated * gated, axis=1, keepdims=True)
            out[span, cols] = (gated * lax.rsqrt(mean + EPS) * gain[:, cols]).astype(bf16)


def output_kernel(attn, mixed, wa, ws, out, *, swapped):
    t = lax.axis_index("tp")
    half = 1 - t if swapped else t
    rows = pl.ds(pl.multiple_of(half * ROWS, ROWS), ROWS)
    out[...] = (dot(attn[rows, :], wa[...]) + dot(mixed[rows, :], ws[...])).astype(bf16)


def total_kernel(kept, received, out):
    rows = pl.ds(pl.multiple_of(pl.program_id(0) * (ROWS // 2), ROWS // 2), ROWS // 2)
    out[...] = (kept[rows, :].astype(f32) + received[rows, :].astype(f32)).astype(bf16)


def call(kernel, name, grid, in_specs, out_specs, out_shape, scratch=(), flops=0, nbytes=0, mib=40):
    return pl.pallas_call(
        kernel,
        name=name,
        grid_spec=pltpu.PrefetchScalarGridSpec(
            num_scalar_prefetch=0,
            grid=grid,
            in_specs=in_specs,
            out_specs=out_specs,
            scratch_shapes=list(scratch),
        ),
        out_shape=out_shape,
        cost_estimate=pl.CostEstimate(flops=flops, transcendentals=0, bytes_accessed=nbytes),
        compiler_params=pltpu.CompilerParams(
            dimension_semantics=("arbitrary",) * len(grid), vmem_limit_bytes=mib << 20
        ),
    )


def local(
    inputs, mix_gain, w_query, w_key, w_value, query_gain, key_gain, sink_logit, w_inner, w_bmat,
    w_cmat, w_gate, w_step, conv_inner, conv_bmat, conv_cmat, step_bias, decay_rate, decay_offset,
    start_state, group_gain, w_out_attn, w_out_state,
):
    sp_count = lax.axis_size("sp")
    swap = [(0, 1), (1, 0)]
    other = lax.ppermute(inputs, "tp", swap)

    cosb, sinb = rotation_tables(np.arange(128) * BLOCK)
    cosi, sini = rotation_tables(np.arange(BLOCK))
    scalar = pl.BlockSpec(memory_space=pltpu.SMEM)
    rows_p = lambda width: pl.BlockSpec((PROWS, width), lambda i: (i, 0))
    step_w = w_step.transpose(1, 2, 0).reshape(16, D)
    widths = (512, 256, 512, 256, 256, 512)
    any_space = pl.BlockSpec(memory_space=pl.ANY)
    part = lambda width: pl.BlockSpec((PART, width), lambda i: (i, 0))
    early = call(
        early_kernel, "early", (1024 // PART,),
        [part(HALF), once((1, D))] + [any_space] * 7 + [once((16, D))],
        [VM] * 14,
        [vmem((1024, 128), f32)]
        + [vmem((1024, width), f32) for width in widths] + [vmem((1024, 16), f32)]
        + [vmem((HALF, width), bf16) for width in widths],
        scratch=[pltpu.VMEM((HALF, width), bf16) for width in widths]
        + [pltpu.VMEM((PART, HALF), bf16), pltpu.SemaphoreType.DMA((14,))],
        flops=1024 * D * 2320, nbytes=20 << 20, mib=24,
    )(
        far(inputs), far(mix_gain.reshape(1, D)), far(w_query), far(w_key), far(w_value),
        far(w_inner), far(w_bmat), far(w_cmat), far(w_gate), far(step_w),
    )
    queries, kv, p1, pc, step_t, gate, lo_edge, hi_edge = call(
        project_kernel, "project", (1024 // PROWS,),
        [
            VM, once((1, D)), once((16, D)), once((1, 64)), once((128, 128)), once((128, 128)),
            once((128, 128)), once((128, 128)),
        ]
        + [VM] * 14,
        [
            VM, rows_p(256), VM, rows_p(256), pl.BlockSpec((16, PROWS), lambda i: (0, i)),
            rows_p(512), whole((192, 256)), whole((192, 256)),
        ],
        [
            vmem((1024, 512), bf16), hbm((1024, 256), bf16), vmem((1024, 768), bf16),
            hbm((1024, 256), bf16), hbm((16, 1024), f32), hbm((1024, 512), bf16), sds((192, 256), bf16),
            sds((192, 256), bf16),
        ],
        scratch=[
            pltpu.VMEM((1, PROWS, 128), f32), pltpu.VMEM((1, PROWS, 128), bf16),
            pltpu.VMEM((PROWS, HALF), bf16),
        ],
        flops=1024 * D * 2320, nbytes=20 << 20, mib=36,
    )(
        near(other), far(mix_gain.reshape(1, D)), far(step_w), far(key_gain.reshape(1, HEAD)),
        far(cosb), far(sinb), far(cosi), far(sini), *[near(value) for value in early],
    )

    forward = [(i, i + 1) for i in range(sp_count - 1)]
    backward = [(i + 1, i) for i in range(sp_count - 1)]
    lo = lax.ppermute(hi_edge, "sp", forward)
    hi = lax.ppermute(lo_edge, "sp", backward)

    rows, col, q_rot = call(
        steps_kernel, "steps", (1,),
        [whole((16, 1024)), scalar, scalar, whole((16, 1024)), VM, whole((1, 64))]
        + [whole((128, 128))] * 4,
        [whole((8, 24, 128)), whole((1024, 128)), whole((1024, 512))],
        [hbm((8, 24, 128), f32), hbm((1024, 128), f32), hbm((1024, 512), bf16)],
        scratch=[pltpu.VMEM((4, 1024, 128), f32), pltpu.VMEM((4, 1024, 128), bf16)],
        flops=1 << 28, nbytes=3 << 20,
    )(
        far(step_t), step_bias, decay_rate, far(decay_offset.reshape(1024, 16).T), near(queries),
        far(query_gain.reshape(1, HEAD)), far(cosb), far(sinb), far(cosi), far(sini),
    )

    lane = np.arange(1024)
    unit = lane // HEAD
    expand = np.zeros((128, 2048), np.float32)
    for u in range(16):
        for base, shift in ((16, 0), (32, 0), (48, 1024), (64, 1024)):
            expand[base + u, shift : shift + 1024] = unit == u
    expand = jnp.asarray(expand, bf16)

    count = SPAN // BLOCK
    blocks = (1024 // SPAN,)
    rows1 = lambda width: pl.BlockSpec((SPAN, width), lambda b: (b, 0))
    rows_m = lambda width: pl.BlockSpec((MSPAN, width), lambda b: (b, 0))
    inner, bmat, add, tot, pack = call(
        mixer_kernel, "mixer", (1024 // MSPAN,),
        [
            VM, VM, VM, once((CONV, 512)), once((CONV, 256)), rows_m(128), once((128, 2048)),
        ],
        [
            rows_m(512), rows_m(256), pl.BlockSpec((MSPAN // BLOCK, 2, 128, 512), lambda b: (b, 0, 0, 0)),
            whole((8, 1024)), whole((16, 16, 640)),
        ],
        [
            hbm((1024, 512), bf16), hbm((1024, 256), bf16), hbm((8, 2, 128, 512), bf16),
            hbm((8, 1024), f32), sds((16, 16, 640), bf16),
        ],
        scratch=[
            pltpu.VMEM((6, MSPAN + 16, 128), f32), pltpu.VMEM((128, 512), f32),
            pltpu.VMEM((128, 512), f32), pltpu.VMEM((1, 512), f32), pltpu.VMEM((1, 512), f32),
            pltpu.VMEM((MSPAN, 1024), bf16), pltpu.VMEM((MSPAN // BLOCK, 2, 128, 512), f32),
        ],
        flops=1 << 30, nbytes=12 << 20,
    )(near(p1), near(lo), near(hi), conv_inner, conv_bmat, far(col), far(expand))

    arrived = lax.all_to_all(pack, "sp", 0, 0, tiled=True)
    wide_rows = pl.BlockSpec((ASPAN, 512), lambda i: (i, 0))
    attention = call(
        attend_kernel, "attend", (1024 // ASPAN,),
        [wide_rows, once((1024, 256)), VM, VM, scalar], wide_rows, hbm((1024, 512), bf16),
        scratch=[
            pltpu.VMEM((2, 1280, 128), bf16), pltpu.VMEM((2, 128, 1280), bf16),
            pltpu.VMEM((ASPAN // 32, 384, 256), f32), pltpu.VMEM((ASPAN // 32, 384, 256), bf16),
        ],
        flops=1 << 31, nbytes=4 << 20,
    )(far(q_rot), far(kv), near(lo), near(hi), sink_logit)
    start_t = start_state.reshape(2, 512, 16, 8).transpose(0, 2, 3, 1)
    arrived, attention, start_t = lax.optimization_barrier((arrived, attention, start_t))
    carried = call(
        carry_kernel, "carry", (1,), [VM, any_space],
        whole((16, 16, 512)), sds((16, 16, 512), bf16),
        scratch=[
            pltpu.VMEM((16, 16, 512), f32), pltpu.VMEM((16, 16, 512), f32),
            pltpu.VMEM((2, 8, 512), f32), pltpu.SemaphoreType.DMA(()),
        ],
        flops=1 << 22, nbytes=1 << 20,
    )(near(arrived), far(start_t))
    carried, pc, inner, bmat, add = lax.optimization_barrier((carried, pc, inner, bmat, add))
    second_half = pl.BlockSpec((128, 1024), lambda b: (0, 1), pipeline_mode=pl.Buffered(1))
    returned = lax.all_to_all(carried, "sp", 0, 0, tiled=True)
    within, cmat = call(
        within_kernel, "within", blocks,
        [
            once((1024, 256)), VM, VM, once((CONV, 256)),
            pl.BlockSpec((count, 24, 128), lambda b: (b, 0, 0)), rows1(128), rows1(512), rows1(256),
            once((8, 2, 128, 512)), once((8, 1024)), second_half,
        ],
        [rows1(512), rows1(256)], [hbm((1024, 512), f32), hbm((1024, 256), bf16)],
        scratch=[
            pltpu.VMEM((2, SPAN + 16, 128), f32), pltpu.VMEM((count, 2, 128, 128), f32),
            pltpu.VMEM((count, 4, 128, 256), bf16), pltpu.VMEM((8, 128, 1024), bf16),
            pltpu.VMEM((SPAN, 1024), f32),
        ],
        flops=1 << 30, nbytes=8 << 20,
    )(
        far(pc), near(lo), near(hi), far(conv_cmat), far(rows), far(col), far(inner), far(bmat),
        far(add), far(tot), far(expand),
    )
    returned, within, cmat = lax.optimization_barrier((returned, within, cmat))
    rows_f = lambda width: pl.BlockSpec((FSPAN, width), lambda b: (b, 0))
    state_out = call(
        finish_kernel, "finish", (1024 // FSPAN,),
        [
            VM, once((8, 1024)), rows_f(512), rows_f(256), rows_f(512), rows_f(128), second_half,
            once((1, 512)),
        ],
        rows_f(512), sds((1024, 512), bf16),
        scratch=[
            pltpu.VMEM((128, 1024), bf16), pltpu.VMEM((8, 1024), f32),
            pltpu.VMEM((FSPAN, 1024), f32),
        ],
        flops=1 << 29, nbytes=10 << 20, mib=24,
    )(
        near(returned), far(tot), far(within), far(cmat), far(gate), far(col),
        far(expand), group_gain.reshape(1, 512),
    )

    def projected(swapped):
        weight = pl.BlockSpec((512, 1024), lambda n: (0, n))
        return call(
            functools.partial(output_kernel, swapped=swapped), "output", (2,),
            [once((1024, 512)), once((1024, 512)), weight, weight],
            pl.BlockSpec((ROWS, 1024), lambda n: (0, n)), sds((ROWS, D), bf16),
            flops=2 * 512 * 1024 * D, nbytes=8 << 20, mib=16,
        )(attention, state_out, w_out_attn, w_out_state)

    sent = projected(True)
    received = lax.ppermute(sent, "tp", swap)
    kept = projected(False)
    return call(
        total_kernel, "total", (2,), [VM, VM], pl.BlockSpec((ROWS // 2, D), lambda i: (i, 0)),
        sds((ROWS, D), bf16), flops=1 << 20, nbytes=6 << 20, mib=8,
    )(near(kept), near(received))


def solution(mesh):
    return jax.shard_map(
        local,
        mesh=mesh,
        in_specs=(
            P(("fs", "sp"), "tp"), P(), P(None, "tp"), P(None, "tp"), P(None, "tp"), P(), P(),
            P("tp"), P(None, "tp"), P(None, "tp"), P(None, "tp"), P(None, "tp"),
            P(None, None, "tp"), P(None, "tp"), P(None, "tp"), P(None, "tp"), P(None, "tp"),
            P(None, "tp"), P("sp", None, "tp"), P("fs", "tp", None, None), P("tp"),
            P("tp", None), P("tp", None),
        ),
        out_specs=P(("fs", "sp", "tp"), None),
        check_vma=False,
    )
```

```python
import functools

import jax
import jax.numpy as jnp
import numpy as np
from jax import lax
from jax.experimental import pallas as pl
from jax.experimental.pallas import tpu as pltpu
from jax.sharding import PartitionSpec as P

D = 2048
HALF = 1024
HEAD = 64
STATE = 128
CONV = 5
BLOCK = 128
EPS = 1e-06
BASE = 10000.0
HEADS = 8
LOG2E = 1.4426950408889634
ROWS = 512
PART = 512
SPAN = 256
ASPAN = 512
MSPAN = 256
PROWS = 1024
FSPAN = 512
f32 = jnp.float32
bf16 = jnp.bfloat16


def dot(a, b):
    return jnp.dot(a, b, preferred_element_type=f32)


def dot_rt(a, b):
    return lax.dot_general(a, b, (((1,), (1,)), ((), ())), preferred_element_type=f32)


def split2(v):
    hi = v.astype(bf16).astype(f32)
    return hi, (v - hi).astype(bf16).astype(f32)


def split3(v):
    hi = v.astype(bf16).astype(f32)
    rest = v - hi
    mid = rest.astype(bf16).astype(f32)
    return hi, mid, (rest - mid).astype(bf16).astype(f32)


def iota(shape, dim):
    return lax.broadcasted_iota(jnp.int32, shape, dim)


def whole(shape):
    zeros = (0,) * len(shape)
    return pl.BlockSpec(shape, lambda *_: zeros)


def once(shape):
    zeros = (0,) * len(shape)
    return pl.BlockSpec(shape, lambda *_: zeros, pipeline_mode=pl.Buffered(1))


def near(value):
    return pltpu.with_memory_space_constraint(value, pltpu.VMEM)


def far(value):
    return pltpu.with_memory_space_constraint(value, pltpu.HBM)


VM = pl.BlockSpec(memory_space=pltpu.VMEM)


def hbm(shape, dtype):
    return pltpu.HBM(shape, dtype)


def vmem(shape, dtype):
    return pltpu.VMEM(shape, dtype)


def sds(shape, dtype):
    return jax.ShapeDtypeStruct(shape, dtype)


def rotation_tables(positions):
    lane = np.arange(128) % 32
    freq = BASE ** (-lane.astype(np.float64) / 32)
    angles = positions.astype(np.float64)[:, None] * freq[None, :]
    return np.cos(angles).astype(np.float32), np.sin(angles).astype(np.float32)


def early_kernel(
    xo, gain, wq, wk, wv, wi, wb, wc, wg, ws,
    ss_o, aq, akv, ai, ab, ac, ag, at, pq, pkv, pi, pb, pc, pg,
    oq, okv, oi, ob, oc, og, xs_o, sems,
):
    i = pl.program_id(0)
    t = lax.axis_index("tp")
    own = pl.multiple_of(t * HALF, HALF)
    peer = pl.multiple_of((1 - t) * HALF, HALF)

    def copies(first, targets, base):
        q, kv, inner, bm, cm, gm = targets
        pairs = (
            (wq, q), (wk, kv.at[:, 0:128]), (wv, kv.at[:, 128:256]), (wi, inner), (wb, bm),
            (wc, cm), (wg, gm),
        )
        return [
            pltpu.make_async_copy(w.at[pl.ds(first, HALF), :], target, sems.at[base + n])
            for n, (w, target) in enumerate(pairs)
        ]

    mine = copies(own, (oq, okv, oi, ob, oc, og), 0)
    others = copies(peer, (pq, pkv, pi, pb, pc, pg), 7)

    @pl.when(i == 0)
    def _():
        for copy in mine:
            copy.start()

    own_x = xo[...].astype(f32)
    rows = pl.ds(pl.multiple_of(i * PART, PART), PART)
    xs_o[...] = (own_x * gain[:, pl.ds(own, HALF)]).astype(bf16)
    ss_o[rows, :] = jnp.broadcast_to(jnp.sum(own_x * own_x, axis=1, keepdims=True), (PART, 128))

    @pl.when(i == 0)
    def _():
        for copy in mine:
            copy.wait()

    for w, acc in ((oq, aq), (okv, akv), (oi, ai), (ob, ab), (oc, ac), (og, ag)):
        acc[rows, :] = dot(xs_o[...], w[...])
    at[rows, :] = dot_rt(xs_o[...], ws[:, pl.ds(own, HALF)])

    @pl.when(i == 0)
    def _():
        for copy in others:
            copy.start()

    @pl.when(i == pl.num_programs(0) - 1)
    def _():
        for copy in others:
            copy.wait()


def swapped(value):
    first = (iota((1, 128), 1) % HEAD) < (HEAD // 2)
    return jnp.where(first, pltpu.roll(value, 96, 1), pltpu.roll(value, 32, 1))


def norm_and_rotate(tiles, outs, gain, first_block, tables, means, scaled):
    cosb, sinb, cosi, sini = tables
    same = (iota((128, 128), 0) // HEAD) == (iota((128, 128), 1) // HEAD)
    averaging = jnp.where(same, 1.0 / HEAD, 0.0).astype(bf16)
    for j, tile in enumerate(tiles):
        values = tile[...].astype(f32)
        scaled[j] = (values * values).astype(bf16)
    for j in range(len(tiles)):
        means[j] = dot(scaled[j], averaging)
    first = (iota((1, 128), 1) % HEAD) < (HEAD // 2)
    wide = jnp.broadcast_to(jnp.concatenate([gain, gain], axis=1), (8, 128))
    gain_a, gain_b = wide[0:1], swapped(wide)[0:1]
    for s in range(tiles[0].shape[0] // BLOCK):
        span = slice(BLOCK * s, BLOCK * (s + 1))
        cb = cosb[pl.ds(first_block + s, 1), :]
        sb = sinb[pl.ds(first_block + s, 1), :]
        cosine = (cb * cosi[...] - sb * sini[...]) * gain_a
        sine = (sb * cosi[...] + cb * sini[...]) * gain_b
        sine = jnp.where(first, -sine, sine)
        for j, tile in enumerate(tiles):
            y = tile[span, :].astype(f32)
            y = (y * cosine + swapped(y) * sine) * lax.rsqrt(means[j, span, :] + EPS)
            outs[j][span, :] = y.astype(bf16)


def project_kernel(
    xp, gain, ws, kg, cosb, sinb, cosi, sini,
    ss, aq, akv, ai, ab, ac, ag, at, wq, wkv, wi, wb, wc, wg,
    q_o, kv_o, p1_o, pc_o, st_o, gate_o, lo_o, hi_o, means, scaled, xs_o,
):
    i = pl.program_id(0)
    t = lax.axis_index("tp")
    sp = lax.axis_index("sp")
    peer = pl.multiple_of((1 - t) * HALF, HALF)
    rows = pl.ds(pl.multiple_of(i * PROWS, PROWS), PROWS)
    peer_x = xp[rows, :].astype(f32)
    xs_o[...] = (peer_x * gain[:, pl.ds(peer, HALF)]).astype(bf16)
    squares = ss[rows, 0:1] + jnp.sum(peer_x * peer_x, axis=1, keepdims=True)
    rs = lax.rsqrt(squares * (1.0 / D) + EPS)

    def proj(w, acc):
        return (dot(xs_o[...], w[...]) + acc[rows, :]) * rs

    kv_o[...] = proj(wkv, akv).astype(bf16)
    p1_o[rows, 0:512] = proj(wi, ai).astype(bf16)
    tile = [kv_o.at[:, 0:128]]
    p1_o[rows, 512:768] = proj(wb, ab).astype(bf16)
    pc_o[...] = proj(wc, ac).astype(bf16)
    q_o[rows, :] = proj(wq, aq).astype(bf16)
    gate_o[...] = proj(wg, ag).astype(bf16)
    block = sp * 8 + i * (PROWS // BLOCK)
    norm_and_rotate(tile, tile, kg[...], block, (cosb, sinb, cosi, sini), means, scaled)
    steps = (dot_rt(xs_o[...], ws[:, pl.ds(peer, HALF)]) + at[rows, :]) * rs
    st_o[...] = jnp.concatenate([steps, jnp.zeros((PROWS, 112), f32)], axis=1).T[0:16, :]

    @pl.when(i == 0)
    def _():
        lo_o[0:128, :] = kv_o[0:128, :]
        for j in range(3):
            lo_o[128 + 16 * j : 144 + 16 * j, :] = p1_o[0:16, 256 * j : 256 * (j + 1)]
        lo_o[176:192, :] = pc_o[0:16, :]

    @pl.when(i == pl.num_programs(0) - 1)
    def _():
        hi_o[0:128, :] = kv_o[PROWS - 128 : PROWS, :]
        for j in range(3):
            hi_o[128 + 16 * j : 144 + 16 * j, :] = p1_o[
                1024 - 16 : 1024, 256 * j : 256 * (j + 1)
            ]
        hi_o[176:192, :] = pc_o[PROWS - 16 : PROWS, :]


def steps_kernel(
    st, bias, rate, offset, q, qg, cosb, sinb, cosi, sini, rows_o, col_o, q_o, means, scaled
):
    tiles = [q.at[:, 128 * j : 128 * (j + 1)] for j in range(4)]
    outs = [q_o.at[:, 128 * j : 128 * (j + 1)] for j in range(4)]
    gain = qg[...] * (HEAD**-0.5 * LOG2E)
    first_block = lax.axis_index("sp") * 8
    norm_and_rotate(tiles, outs, gain, first_block, (cosb, sinb, cosi, sini), means, scaled)
    unit = iota((16, 1), 0)

    def as_column(table):
        value = jnp.zeros((16, 1), f32)
        for d in range(2):
            for h in range(HEADS):
                value = jnp.where(unit == 8 * d + h, table[d, h], value)
        return value

    v = st[...] + as_column(bias)
    step = jnp.maximum(v, 0.0) + jnp.log1p(jnp.exp(-jnp.abs(v)))
    decay = -as_column(rate) * step + offset[...]
    count = 1024 // BLOCK
    parts = [decay[:, BLOCK * s : BLOCK * (s + 1)] for s in range(count)]
    stacked = jnp.concatenate(parts, axis=0)
    hi, mid, lo = split3(stacked)
    row = iota((128, 256), 0)
    column = iota((128, 256), 1)
    prefix = (column < 128) & (row <= column)
    suffix = (column >= 128) & (row >= column - 128)
    sums = jnp.where(prefix | suffix, 1.0, 0.0).astype(bf16)
    total = dot(hi.astype(bf16), sums) + dot(mid.astype(bf16), sums) + dot(lo.astype(bf16), sums)
    for s in range(count):
        c = jnp.concatenate(
            [total[16 * s : 16 * s + 8, 0:128], total[16 * s + 8 : 16 * s + 16, 128:256]], axis=0
        )
        steps = step[:, BLOCK * s : BLOCK * (s + 1)]
        last = jnp.concatenate([c[0:8, 127:128], c[8:16, 0:1]], axis=0)
        factor = steps * jnp.exp(last - c)
        raised = jnp.exp(c)
        rows_o[s, 0:16, :] = (jnp.log(steps) - c) * LOG2E
        rows_o[s, 16:24, :] = steps[0:8] + steps[8:16]
        factor_hi, factor_lo = split2(factor)
        raised_hi, raised_lo = split2(raised)
        packed = jnp.concatenate(
            [c * LOG2E, factor_hi, factor_lo, raised_hi, raised_lo, jnp.zeros((48, 128), f32)],
            axis=0,
        )
        col_o[BLOCK * s : BLOCK * (s + 1), :] = packed.T


def frame(p1, lo, hi, xpad, first_piece):
    i = pl.program_id(0)
    rows = xpad.shape[1] - 16
    start = pl.multiple_of(i * rows, rows)
    final = pl.num_programs(0) - 1
    chunks = xpad.shape[0]
    after_rows = slice(rows + 8, rows + 16)

    @pl.when(i == 0)
    def _():
        for c in range(chunks):
            top = 128 + 16 * (first_piece + c // 2)
            lanes = slice(128 * (c % 2), 128 * (c % 2) + 128)
            xpad[c, 0:8, :] = lo[top : top + 16, lanes].astype(f32)[8:16]

    @pl.when(i > 0)
    def _():
        before = pl.multiple_of(jnp.maximum(start - 16, 0), 16)
        rim = p1[pl.ds(before, 16), :].astype(f32)[8:16]
        for c in range(chunks):
            xpad[c, 0:8, :] = rim[:, 128 * c : 128 * (c + 1)]

    @pl.when(i < final)
    def _():
        after = pl.multiple_of(jnp.minimum(start + rows, 1008), 16)
        rim = p1[pl.ds(after, 16), :].astype(f32)[0:8]
        for c in range(chunks):
            xpad[c, after_rows, :] = rim[:, 128 * c : 128 * (c + 1)]

    @pl.when(i == final)
    def _():
        for c in range(chunks):
            top = 128 + 16 * (first_piece + c // 2)
            lanes = slice(128 * (c % 2), 128 * (c % 2) + 128)
            xpad[c, after_rows, :] = hi[top : top + 16, lanes].astype(f32)[0:8]

    for c in range(chunks):
        xpad[c, 8 : rows + 8, :] = p1[pl.ds(start, rows), 128 * c : 128 * (c + 1)].astype(f32)


def convolve(xpad, taps, chunk, out):
    table = taps[...].astype(f32)
    rows = xpad.shape[1] - 16
    for c in range(taps.shape[1] // 128):
        lanes = slice(128 * c, 128 * (c + 1))
        total = table[0:1, lanes] * xpad[chunk + c, 6 : 6 + rows, :]
        for j in range(1, CONV):
            total = total + table[j : j + 1, lanes] * xpad[chunk + c, 6 + j : 6 + j + rows, :]
        out[:, lanes] = (total / (1.0 + jnp.exp(-total))).astype(bf16)


def mixer_kernel(
    p1, lo, hi, ti, tb, col, expand,
    inner_s, bs, add_o, tot_o, pack_o,
    xpad, run_f, run_b, prod_f, prod_b, loaded, added,
):
    i = pl.program_id(0)

    @pl.when(i == 0)
    def _():
        run_f[...] = jnp.zeros_like(run_f)
        run_b[...] = jnp.zeros_like(run_b)
        prod_f[...] = jnp.ones_like(prod_f)
        prod_b[...] = jnp.ones_like(prod_b)

    frame(p1, lo, hi, xpad, 0)
    count = MSPAN // BLOCK
    spans = [slice(BLOCK * k, BLOCK * (k + 1)) for k in range(count)]
    groups = [slice(128 * g, 128 * (g + 1)) for g in range(2)]
    convolve(xpad, tb, 4, bs)
    flipped = bs[...].astype(f32).T.astype(bf16)
    convolve(xpad, ti, 0, inner_s)
    factors = col[...].astype(bf16)
    tot_f, tot_b = [], []
    for k in range(count):
        widened = dot(factors[spans[k], :], expand[:, 0:1024])
        end = dot(factors[BLOCK * k + 112 : BLOCK * k + 128, :], expand[:, 1024:1536])
        begin = dot(factors[BLOCK * k : BLOCK * k + 16, :], expand[:, 1536:2048])
        inner_wide = inner_s[spans[k], :].astype(f32)
        loaded[spans[k], 0:512] = (inner_wide * widened[:, 0:512]).astype(bf16)
        loaded[spans[k], 512:1024] = (inner_wide * widened[:, 512:1024]).astype(bf16)
        tot_f.append(end[15:16])
        tot_b.append(begin[0:1])
        tot_o[pl.ds(i * count + k, 1), 0:512] = tot_f[k]
        tot_o[pl.ds(i * count + k, 1), 512:1024] = tot_b[k]
    for k in range(count):
        for g in range(2):
            for d in range(2):
                cols = slice(256 * g, 256 * (g + 1))
                cols_d = slice(512 * d + 256 * g, 512 * d + 256 * (g + 1))
                added[k, d, :, cols] = dot(flipped[groups[g], spans[k]], loaded[spans[k], cols_d])
    for k in range(count):
        for c in range(4):
            cols = slice(128 * c, 128 * (c + 1))
            run_f[:, cols] = tot_f[k][:, cols] * run_f[:, cols] + added[k, 0, :, cols]
            run_b[:, cols] = run_b[:, cols] + prod_b[:, cols] * added[k, 1, :, cols]
        add_o[k] = added[k].astype(bf16)
        prod_f[...] = prod_f[...] * tot_f[k]
        prod_b[...] = prod_b[...] * tot_b[k]

    @pl.when(i == pl.num_programs(0) - 1)
    def _():
        levels = jnp.concatenate([prod_f[...], prod_b[...]], axis=0)
        hi_l, mid_l, lo_l = split3(levels)
        joined = jnp.concatenate([hi_l, mid_l, lo_l], axis=1).astype(bf16)
        lane = iota((1536, 128), 0)
        head = iota((1536, 128), 1)
        wanted = (lane // 512) * 8 + (lane % 512) // HEAD
        pick = jnp.where((lane % HEAD == 0) & (head == wanted), 1.0, 0.0).astype(bf16)
        sent = dot(joined, pick)
        sent = jnp.concatenate(
            [jnp.broadcast_to(sent[0:1], (8, 128)), jnp.broadcast_to(sent[1:2], (8, 128))], axis=0
        ).astype(bf16)
        for j in range(16):
            pack_o[j, :, 0:512] = jnp.concatenate(
                [run_f[8 * j : 8 * j + 8, :], run_b[8 * j : 8 * j + 8, :]], axis=0
            ).astype(bf16)
            pack_o[j, :, 512:640] = sent


def within_kernel(
    pc, lo, hi, tc, rows, col, inner, bmat, add, tot, expand,
    within_o, cmat_o, xpad, score, weight, begun, made,
):
    i = pl.program_id(0)

    @pl.when(i == 0)
    def _():
        for d in range(2):
            for c in range(4):
                cols = slice(128 * c, 128 * (c + 1))
                cols_d = slice(512 * d + 128 * c, 512 * d + 128 * (c + 1))
                state = jnp.zeros((128, 128), f32)
                for b in range(8) if d == 0 else reversed(range(8)):
                    begun[b, :, cols_d] = state.astype(bf16)
                    if b != (7 if d == 0 else 0):
                        state = tot[b : b + 1, cols_d] * state + add[b, d, :, cols].astype(f32)

    frame(pc, lo, hi, xpad, 3)
    convolve(xpad, tc, 0, cmat_o)
    count = SPAN // BLOCK
    spans = [slice(BLOCK * k, BLOCK * (k + 1)) for k in range(count)]
    groups = [slice(128 * g, 128 * (g + 1)) for g in range(2)]
    for k in range(count):
        for g in range(2):
            score[k, g] = dot_rt(cmat_o[spans[k], groups[g]], bmat[spans[k], groups[g]])
    for k in range(count):
        for g in range(2):
            both = jnp.concatenate(
                [
                    begun[i * count + k, :, 256 * g : 256 * (g + 1)],
                    begun[i * count + k, :, 512 + 256 * g : 512 + 256 * (g + 1)],
                ],
                axis=1,
            )
            both = dot(cmat_o[spans[k], groups[g]], both)
            made[spans[k], 256 * g : 256 * (g + 1)] = both[:, 0:256]
            made[spans[k], 512 + 256 * g : 512 + 256 * (g + 1)] = both[:, 256:512]
    for k in range(count):
        widened = dot(col[spans[k], :].astype(bf16), expand[...])
        within_o[spans[k], :] = (
            widened[:, 0:512] * made[spans[k], 0:512]
            + widened[:, 512:1024] * made[spans[k], 512:1024]
        )
    row = iota((128, 128), 0)
    column = iota((128, 128), 1)
    causal = row >= column
    diagonal = row == column
    for k in range(count):
        for h in range(HEADS):
            forward = col[spans[k], h : h + 1] + rows[k, h : h + 1, :]
            backward = col[spans[k], 8 + h : 9 + h] + rows[k, 8 + h : 9 + h, :]
            spread = jnp.exp2(jnp.where(causal, forward, backward))
            spread = jnp.where(diagonal, rows[k, 16 + h : 17 + h, :], spread)
            weight[k, h // 2, :, 128 * (h % 2) : 128 * (h % 2) + 128] = (
                score[k, h // 4] * spread
            ).astype(bf16)
    low_lane = iota((1, 128), 1) < HEAD
    for k in range(count):
        for pair in range(HEADS // 2):
            both = inner[spans[k], 128 * pair : 128 * (pair + 1)]
            zero = jnp.zeros_like(both)
            right = jnp.concatenate(
                [jnp.where(low_lane, both, zero), jnp.where(low_lane, zero, both)], axis=0
            )
            cols = slice(128 * pair, 128 * (pair + 1))
            within_o[spans[k], cols] = within_o[spans[k], cols] + dot(weight[k, pair], right)


def carry_kernel(arrived, start, out, wide, held, first, sem):
    fetch = pltpu.make_async_copy(start.at[:, lax.axis_index("sp")], first, sem)
    fetch.start()
    lane = iota((128, 512), 0)
    spread = (lane < 24) & (iota((128, 512), 1) // HEAD == lane % 8)
    spread = jnp.where(spread, 1.0, 0.0).astype(bf16)
    for j in range(16):
        wide[j] = dot(arrived[j, :, 512:640], spread)
    fetch.wait()
    state = first[0]
    for j in range(16):
        held[j, 0:8, :] = state
        state = wide[j, 0:8, :] * state + arrived[j, :, 0:512].astype(f32)[0:8]
    state = first[1]
    for j in reversed(range(16)):
        held[j, 8:16, :] = state
        state = wide[j, 8:16, :] * state + arrived[j, :, 0:512].astype(f32)[8:16]
    for j in range(16):
        out[j] = held[j].astype(bf16)


def attend_kernel(q, kv, lo, hi, sink, out, keys, vals, score, weight):
    i = pl.program_id(0)
    sp = lax.axis_index("sp")
    low_lane = iota((1, 128), 1) < HEAD

    def place(first, count, pairs):
        kk = pairs[:, 0:128].astype(f32)
        kr = pltpu.roll(kk, 64, 1)
        span = slice(first, first + count)
        keys[0, span, :] = jnp.where(low_lane, kk, kr).astype(bf16)
        keys[1, span, :] = jnp.where(low_lane, kr, kk).astype(bf16)
        flipped = pairs[:, 128:256].astype(f32).T.astype(bf16)
        ones = jnp.ones((HEAD, count), bf16)
        for g in range(2):
            vals[g, 0:HEAD, span] = flipped[HEAD * g : HEAD * (g + 1)]
            vals[g, HEAD:128, span] = ones

    @pl.when(i == 0)
    def _():
        place(0, 128, lo[0:128, :])
        place(128, 1024, kv[...])
        place(1152, 128, hi[0:128, :])

    count = ASPAN // BLOCK
    starts = [pl.multiple_of(i * ASPAN + BLOCK * k, BLOCK) for k in range(count)]
    items = [(k, g, j) for k in range(count) for g in range(2) for j in range(2)]
    for n, (k, g, j) in enumerate(items):
        base = 256 * g + 128 * j
        tile = q[BLOCK * k : BLOCK * (k + 1), base : base + 128]
        zero = jnp.zeros_like(tile)
        both = jnp.concatenate(
            [jnp.where(low_lane, tile, zero), jnp.where(low_lane, zero, tile)], axis=0
        )
        score[n] = dot_rt(keys[g, pl.ds(starts[k], 384), :], both)
    key = iota((128, 128), 0)
    query = iota((128, 128), 1)
    biases = []
    for k in range(count):
        b = i * count + k
        no_left = (b == 0) & (sp == 0)
        no_right = (b == 7) & (sp == lax.axis_size("sp") - 1)
        left_from = jnp.where(no_left, 128, 0)
        right_to = jnp.where(no_right, -1, 127)
        left = jnp.where((key >= query) & (key >= left_from), 0.0, -1e30)
        right = jnp.where((key <= query) & (key <= right_to), 0.0, -1e30)
        biases.append((left, right))
    sinks = []
    for n, (k, g, j) in enumerate(items):
        left, right = biases[k]
        for half in range(2):
            lanes = slice(128 * half, 128 * (half + 1))
            sink_h = jnp.full((1, 128), sink[4 * g + 2 * j + half] * LOG2E, f32)
            low = score[n, 0:128, lanes] + left
            middle = score[n, 128:256, lanes]
            high = score[n, 256:384, lanes] + right
            highest = jnp.max(jnp.maximum(jnp.maximum(low, middle), high), axis=0, keepdims=True)
            highest = jnp.maximum(highest, sink_h)
            weight[n, 0:128, lanes] = jnp.exp2(low - highest).astype(bf16)
            weight[n, 128:256, lanes] = jnp.exp2(middle - highest).astype(bf16)
            weight[n, 256:384, lanes] = jnp.exp2(high - highest).astype(bf16)
            sinks.append(jnp.exp2(sink_h - highest))
    results = [
        dot(vals[g, :, pl.ds(starts[k], 384)], weight[n]) for n, (k, g, j) in enumerate(items)
    ]
    for n, (k, g, j) in enumerate(items):
        finals = []
        for half in range(2):
            lanes = slice(128 * half, 128 * (half + 1))
            denominator = results[n][HEAD : HEAD + 1, lanes] + sinks[2 * n + half]
            finals.append(results[n][0:HEAD, lanes] * (1.0 / denominator))
        base = 256 * g + 128 * j
        out[BLOCK * k : BLOCK * (k + 1), base : base + 128] = (
            jnp.concatenate(finals, axis=0).T.astype(bf16)
        )


def finish_kernel(arrived, tot, within, cmat, gate, col, expand, gain, out, entering, kept, made):
    i = pl.program_id(0)

    @pl.when(i == 0)
    def _():
        for j in range(16):
            slab = arrived[j].astype(f32)
            made[8 * j : 8 * j + 8, 0:512] = slab[0:8]
            made[8 * j : 8 * j + 8, 512:1024] = slab[8:16]
        entering[...] = made[0:128, :].astype(bf16)
        level = jnp.ones((1, 512), f32)
        for b in range(8):
            kept[b : b + 1, 0:512] = level
            level = level * tot[b : b + 1, 0:512]
        level = jnp.ones((1, 512), f32)
        for b in reversed(range(8)):
            kept[b : b + 1, 512:1024] = level
            level = level * tot[b : b + 1, 512:1024]

    count = FSPAN // BLOCK
    for g in range(2):
        for d in range(2):
            cols = slice(512 * d + 256 * g, 512 * d + 256 * (g + 1))
            made[:, cols] = dot(cmat[:, 128 * g : 128 * (g + 1)], entering[:, cols])
    for k in range(count):
        span = slice(BLOCK * k, BLOCK * (k + 1))
        widened = dot(col[span, :].astype(bf16), expand[...]) * kept[pl.ds(i * count + k, 1), :]
        for g in range(2):
            cols = slice(256 * g, 256 * (g + 1))
            cols_b = slice(512 + 256 * g, 512 + 256 * (g + 1))
            total = within[span, cols] + widened[:, cols] * made[span, cols]
            total = total + widened[:, cols_b] * made[span, cols_b]
            gates = gate[span, cols].astype(f32)
            gated = total * (gates / (1.0 + jnp.exp(-gates)))
            mean = jnp.mean(gated * gated, axis=1, keepdims=True)
            out[span, cols] = (gated * lax.rsqrt(mean + EPS) * gain[:, cols]).astype(bf16)


def output_kernel(attn, mixed, wa, ws, out, *, swapped):
    t = lax.axis_index("tp")
    half = 1 - t if swapped else t
    rows = pl.ds(pl.multiple_of(half * ROWS, ROWS), ROWS)
    out[...] = (dot(attn[rows, :], wa[...]) + dot(mixed[rows, :], ws[...])).astype(bf16)


def total_kernel(kept, received, out):
    rows = pl.ds(pl.multiple_of(pl.program_id(0) * (ROWS // 2), ROWS // 2), ROWS // 2)
    out[...] = (kept[rows, :].astype(f32) + received[rows, :].astype(f32)).astype(bf16)


def call(kernel, name, grid, in_specs, out_specs, out_shape, scratch=(), flops=0, nbytes=0, mib=40):
    return pl.pallas_call(
        kernel,
        name=name,
        grid_spec=pltpu.PrefetchScalarGridSpec(
            num_scalar_prefetch=0,
            grid=grid,
            in_specs=in_specs,
            out_specs=out_specs,
            scratch_shapes=list(scratch),
        ),
        out_shape=out_shape,
        cost_estimate=pl.CostEstimate(flops=flops, transcendentals=0, bytes_accessed=nbytes),
        compiler_params=pltpu.CompilerParams(
            dimension_semantics=("arbitrary",) * len(grid), vmem_limit_bytes=mib << 20
        ),
    )


def local(
    inputs, mix_gain, w_query, w_key, w_value, query_gain, key_gain, sink_logit, w_inner, w_bmat,
    w_cmat, w_gate, w_step, conv_inner, conv_bmat, conv_cmat, step_bias, decay_rate, decay_offset,
    start_state, group_gain, w_out_attn, w_out_state,
):
    sp_count = lax.axis_size("sp")
    swap = [(0, 1), (1, 0)]
    other = lax.ppermute(inputs, "tp", swap)

    cosb, sinb = rotation_tables(np.arange(128) * BLOCK)
    cosi, sini = rotation_tables(np.arange(BLOCK))
    scalar = pl.BlockSpec(memory_space=pltpu.SMEM)
    rows_p = lambda width: pl.BlockSpec((PROWS, width), lambda i: (i, 0))
    step_w = w_step.transpose(1, 2, 0).reshape(16, D)
    widths = (512, 256, 512, 256, 256, 512)
    any_space = pl.BlockSpec(memory_space=pl.ANY)
    part = lambda width: pl.BlockSpec((PART, width), lambda i: (i, 0))
    early = call(
        early_kernel, "early", (1024 // PART,),
        [part(HALF), once((1, D))] + [any_space] * 7 + [once((16, D))],
        [VM] * 14,
        [vmem((1024, 128), f32)]
        + [vmem((1024, width), f32) for width in widths] + [vmem((1024, 16), f32)]
        + [vmem((HALF, width), bf16) for width in widths],
        scratch=[pltpu.VMEM((HALF, width), bf16) for width in widths]
        + [pltpu.VMEM((PART, HALF), bf16), pltpu.SemaphoreType.DMA((14,))],
        flops=1024 * D * 2320, nbytes=20 << 20, mib=24,
    )(
        far(inputs), far(mix_gain.reshape(1, D)), far(w_query), far(w_key), far(w_value),
        far(w_inner), far(w_bmat), far(w_cmat), far(w_gate), far(step_w),
    )
    queries, kv, p1, pc, step_t, gate, lo_edge, hi_edge = call(
        project_kernel, "project", (1024 // PROWS,),
        [
            VM, once((1, D)), once((16, D)), once((1, 64)), once((128, 128)), once((128, 128)),
            once((128, 128)), once((128, 128)),
        ]
        + [VM] * 14,
        [
            VM, rows_p(256), VM, rows_p(256), pl.BlockSpec((16, PROWS), lambda i: (0, i)),
            rows_p(512), whole((192, 256)), whole((192, 256)),
        ],
        [
            vmem((1024, 512), bf16), hbm((1024, 256), bf16), vmem((1024, 768), bf16),
            hbm((1024, 256), bf16), hbm((16, 1024), f32), hbm((1024, 512), bf16), sds((192, 256), bf16),
            sds((192, 256), bf16),
        ],
        scratch=[
            pltpu.VMEM((1, PROWS, 128), f32), pltpu.VMEM((1, PROWS, 128), bf16),
            pltpu.VMEM((PROWS, HALF), bf16),
        ],
        flops=1024 * D * 2320, nbytes=20 << 20, mib=36,
    )(
        near(other), far(mix_gain.reshape(1, D)), far(step_w), far(key_gain.reshape(1, HEAD)),
        far(cosb), far(sinb), far(cosi), far(sini), *[near(value) for value in early],
    )

    forward = [(i, i + 1) for i in range(sp_count - 1)]
    backward = [(i + 1, i) for i in range(sp_count - 1)]
    lo = lax.ppermute(hi_edge, "sp", forward)
    hi = lax.ppermute(lo_edge, "sp", backward)

    rows, col, q_rot = call(
        steps_kernel, "steps", (1,),
        [whole((16, 1024)), scalar, scalar, whole((16, 1024)), VM, whole((1, 64))]
        + [whole((128, 128))] * 4,
        [whole((8, 24, 128)), whole((1024, 128)), whole((1024, 512))],
        [hbm((8, 24, 128), f32), hbm((1024, 128), f32), hbm((1024, 512), bf16)],
        scratch=[pltpu.VMEM((4, 1024, 128), f32), pltpu.VMEM((4, 1024, 128), bf16)],
        flops=1 << 28, nbytes=3 << 20,
    )(
        far(step_t), step_bias, decay_rate, far(decay_offset.reshape(1024, 16).T), near(queries),
        far(query_gain.reshape(1, HEAD)), far(cosb), far(sinb), far(cosi), far(sini),
    )

    lane = np.arange(1024)
    unit = lane // HEAD
    expand = np.zeros((128, 2048), np.float32)
    for u in range(16):
        for base, shift in ((16, 0), (32, 0), (48, 1024), (64, 1024)):
            expand[base + u, shift : shift + 1024] = unit == u
    expand = jnp.asarray(expand, bf16)

    count = SPAN // BLOCK
    blocks = (1024 // SPAN,)
    rows1 = lambda width: pl.BlockSpec((SPAN, width), lambda b: (b, 0))
    rows_m = lambda width: pl.BlockSpec((MSPAN, width), lambda b: (b, 0))
    inner, bmat, add, tot, pack = call(
        mixer_kernel, "mixer", (1024 // MSPAN,),
        [
            VM, VM, VM, once((CONV, 512)), once((CONV, 256)), rows_m(128), once((128, 2048)),
        ],
        [
            rows_m(512), rows_m(256), pl.BlockSpec((MSPAN // BLOCK, 2, 128, 512), lambda b: (b, 0, 0, 0)),
            whole((8, 1024)), whole((16, 16, 640)),
        ],
        [
            hbm((1024, 512), bf16), hbm((1024, 256), bf16), hbm((8, 2, 128, 512), bf16),
            hbm((8, 1024), f32), sds((16, 16, 640), bf16),
        ],
        scratch=[
            pltpu.VMEM((6, MSPAN + 16, 128), f32), pltpu.VMEM((128, 512), f32),
            pltpu.VMEM((128, 512), f32), pltpu.VMEM((1, 512), f32), pltpu.VMEM((1, 512), f32),
            pltpu.VMEM((MSPAN, 1024), bf16), pltpu.VMEM((MSPAN // BLOCK, 2, 128, 512), f32),
        ],
        flops=1 << 30, nbytes=12 << 20,
    )(near(p1), near(lo), near(hi), conv_inner, conv_bmat, far(col), far(expand))

    arrived = lax.all_to_all(pack, "sp", 0, 0, tiled=True)
    wide_rows = pl.BlockSpec((ASPAN, 512), lambda i: (i, 0))
    attention = call(
        attend_kernel, "attend", (1024 // ASPAN,),
        [wide_rows, once((1024, 256)), VM, VM, scalar], wide_rows, hbm((1024, 512), bf16),
        scratch=[
            pltpu.VMEM((2, 1280, 128), bf16), pltpu.VMEM((2, 128, 1280), bf16),
            pltpu.VMEM((ASPAN // 32, 384, 256), f32), pltpu.VMEM((ASPAN // 32, 384, 256), bf16),
        ],
        flops=1 << 31, nbytes=4 << 20,
    )(far(q_rot), far(kv), near(lo), near(hi), sink_logit)
    start_t = start_state.reshape(2, 512, 16, 8).transpose(0, 2, 3, 1)
    arrived, attention, start_t = lax.optimization_barrier((arrived, attention, start_t))
    carried = call(
        carry_kernel, "carry", (1,), [VM, any_space],
        whole((16, 16, 512)), sds((16, 16, 512), bf16),
        scratch=[
            pltpu.VMEM((16, 16, 512), f32), pltpu.VMEM((16, 16, 512), f32),
            pltpu.VMEM((2, 8, 512), f32), pltpu.SemaphoreType.DMA(()),
        ],
        flops=1 << 22, nbytes=1 << 20,
    )(near(arrived), far(start_t))
    carried, pc, inner, bmat, add = lax.optimization_barrier((carried, pc, inner, bmat, add))
    second_half = pl.BlockSpec((128, 1024), lambda b: (0, 1), pipeline_mode=pl.Buffered(1))
    returned = lax.all_to_all(carried, "sp", 0, 0, tiled=True)
    within, cmat = call(
        within_kernel, "within", blocks,
        [
            once((1024, 256)), VM, VM, once((CONV, 256)),
            pl.BlockSpec((count, 24, 128), lambda b: (b, 0, 0)), rows1(128), rows1(512), rows1(256),
            once((8, 2, 128, 512)), once((8, 1024)), second_half,
        ],
        [rows1(512), rows1(256)], [hbm((1024, 512), f32), hbm((1024, 256), bf16)],
        scratch=[
            pltpu.VMEM((2, SPAN + 16, 128), f32), pltpu.VMEM((count, 2, 128, 128), f32),
            pltpu.VMEM((count, 4, 128, 256), bf16), pltpu.VMEM((8, 128, 1024), bf16),
            pltpu.VMEM((SPAN, 1024), f32),
        ],
        flops=1 << 30, nbytes=8 << 20,
    )(
        far(pc), near(lo), near(hi), far(conv_cmat), far(rows), far(col), far(inner), far(bmat),
        far(add), far(tot), far(expand),
    )
    returned, within, cmat = lax.optimization_barrier((returned, within, cmat))
    rows_f = lambda width: pl.BlockSpec((FSPAN, width), lambda b: (b, 0))
    state_out = call(
        finish_kernel, "finish", (1024 // FSPAN,),
        [
            VM, once((8, 1024)), rows_f(512), rows_f(256), rows_f(512), rows_f(128), second_half,
            once((1, 512)),
        ],
        rows_f(512), sds((1024, 512), bf16),
        scratch=[
            pltpu.VMEM((128, 1024), bf16), pltpu.VMEM((8, 1024), f32),
            pltpu.VMEM((FSPAN, 1024), f32),
        ],
        flops=1 << 29, nbytes=10 << 20, mib=24,
    )(
        near(returned), far(tot), far(within), far(cmat), far(gate), far(col),
        far(expand), group_gain.reshape(1, 512),
    )

    def projected(swapped):
        weight = pl.BlockSpec((512, 1024), lambda n: (0, n))
        return call(
            functools.partial(output_kernel, swapped=swapped), "output", (2,),
            [once((1024, 512)), once((1024, 512)), weight, weight],
            pl.BlockSpec((ROWS, 1024), lambda n: (0, n)), sds((ROWS, D), bf16),
            flops=2 * 512 * 1024 * D, nbytes=8 << 20, mib=16,
        )(attention, state_out, w_out_attn, w_out_state)

    sent = projected(True)
    received = lax.ppermute(sent, "tp", swap)
    kept = projected(False)
    return call(
        total_kernel, "total", (2,), [VM, VM], pl.BlockSpec((ROWS // 2, D), lambda i: (i, 0)),
        sds((ROWS, D), bf16), flops=1 << 20, nbytes=6 << 20, mib=8,
    )(near(kept), near(received))


def solution(mesh):
    return jax.shard_map(
        local,
        mesh=mesh,
        in_specs=(
            P(("fs", "sp"), "tp"), P(), P(None, "tp"), P(None, "tp"), P(None, "tp"), P(), P(),
            P("tp"), P(None, "tp"), P(None, "tp"), P(None, "tp"), P(None, "tp"),
            P(None, None, "tp"), P(None, "tp"), P(None, "tp"), P(None, "tp"), P(None, "tp"),
            P(None, "tp"), P("sp", None, "tp"), P("fs", "tp", None, None), P("tp"),
            P("tp", None), P("tp", None),
        ),
        out_specs=P(("fs", "sp", "tp"), None),
        check_vma=False,
    )
```
